256 devices in a mesh: sp: 64 (over z, y, core), tp: 4 (over x).
Axes of the slice: x: 4, y: 4, z: 8, core: 2. Of those that a mesh axis runs over, the one named last changes fastest.
Arguments:
- head_input_values: bfloat16 [24576, 4096], P('sp', 'tp'), may hold values from -6 to 6
- group_input_vectors: bfloat16 [24576, 1024], P('sp', 'tp'), may hold values from -6 to 6
- group_readout_vectors: bfloat16 [24576, 1024], P('sp', 'tp'), may hold values from -6 to 6
- output_gate_values: bfloat16 [24576, 4096], P('sp', 'tp'), may hold values from -6 to 6
- step_size_logits: float32 [24576, 64], P('sp', 'tp'), may hold values from -6 to 6
- extra_log_decay: float32 [24576, 64], P('sp', 'tp'), may hold values from -1.2 to 0
- head_input_filter: bfloat16 [4, 4096], P(None, 'tp'), may hold values from -3 to 3
- input_vector_filter: bfloat16 [4, 1024], P(None, 'tp'), may hold values from -3 to 3
- readout_vector_filter: bfloat16 [4, 1024], P(None, 'tp'), may hold values from -3 to 3
- step_size_bias: float32 [64], P('tp'), may hold values from -0.5 to 0.5
- head_rate_logarithm: float32 [64], P('tp'), may hold values from -20 to -1
- direct_path_weight: float32 [64], P('tp'), may hold values from 0 to 3
- group_norm_scale: bfloat16 [4096], P('tp'), may hold values from 0.099609375 to 1.8984375
- mixer_output_weight: bfloat16 [4096, 2048], P('tp'), may hold values from -0.09375 to 0.09375
- residual: bfloat16 [24576, 2048], P(('sp', 'tp')), may hold values from -6 to 6
- first_norm_scale: float32 [2048], replicated, may hold values from 0.1 to 1.9
- first_norm_bias: float32 [2048], replicated, may hold values from -1.5 to 1.5
- routes: int32 [24576, 2], P(('sp', 'tp')), may hold values from 0 to 63, all different within a row; in each aligned block of 96 rows (0 to 95, 96 to 191, ...) at most 5 rows name the same one
- routing_weight: float32 [24576, 2], P(('sp', 'tp')), may hold values from 0.1 to 0.9
- expert_gate_weight: bfloat16 [64, 2048, 1024], P('sp', None, 'tp'), may hold values from -0.125 to 0.125
- expert_up_weight: bfloat16 [64, 2048, 1024], P('sp', None, 'tp'), may hold values from -0.125 to 0.125
- expert_down_weight: bfloat16 [64, 2048, 1024], P('sp', None, 'tp'), may hold values from -0.1875 to 0.1875
- final_norm_scale: float32 [2048], replicated, may hold values from 0.1 to 1.9
- final_norm_bias: float32 [2048], replicated, may hold values from -1.5 to 1.5
Outputs:
- final: bfloat16 [24576, 2048], P(('sp', 'tp'))
The draws below stay inside these ranges and needn't reach their ends.
Inputs may be any that keep to these rules, and one draw needn't show every extreme that they name: `routes`: in the rows of one device no expert is named more than 5 times.
All inputs are finite; a program needn't handle non-finite values.
Results may differ from the reference program's by a relative error of at most 0.012.
Values may be sent and summed in bfloat16 or wider, within the bound.
A program may use at most 128 MiB of HBM per device.

```python
import math
import jax
import jax.numpy as jnp
import numpy as np
from jax import lax

D = 2048
HEAD_COUNT = 64
HEAD_DIM = 64
INNER_WIDTH = 4096
GROUP_COUNT = 8
STATE_WIDTH = 128
TAPS = 4
BLOCK_LENGTH = 128
FFE = 1024
TOPK = 2
EXPERTS = 64
TOK_DEV = 384
TOKEN_COUNT = 24576
CAP = 5
N_SP = 64
N_TP = 4


def draw_step_size_logits(key, part):
    key_noise, key_shift, key_heat = jax.random.split(jax.random.fold_in(key, 11), 3)
    block_list = TOKEN_COUNT // TOK_DEV
    heated = jax.random.bernoulli(key_heat, 0.0625, (block_list, 1, HEAD_COUNT))
    jitter = jax.random.uniform(key_shift, (block_list, 1, HEAD_COUNT), jnp.float32, -0.3, 0.3)
    block_shift = jnp.where(heated, 3.5, -1.0) + jitter
    noise_part = 0.7 * jax.random.normal(key_noise, (block_list, TOK_DEV, HEAD_COUNT), jnp.float32)
    return jnp.clip(noise_part + block_shift, -6.0, 6.0).reshape(TOKEN_COUNT, HEAD_COUNT)


def draw_head_rate_logarithm(key, part):
    key_pick, key_fast, key_slow = jax.random.split(jax.random.fold_in(key, 12), 3)
    chance = 0.5
    quick = jax.random.bernoulli(key_pick, chance, (HEAD_COUNT,))
    fast_rate = jnp.log(jax.random.uniform(key_fast, (HEAD_COUNT,), jnp.float32, 0.05, 0.15))
    slow_rate = jnp.log(jax.random.uniform(key_slow, (HEAD_COUNT,), jnp.float32, 0.9, 1.4)) - jnp.log(jnp.float32(0.6 * TOKEN_COUNT))
    return jnp.where(quick, fast_rate, slow_rate)


def draw_extra_log_decay(key, part):
    random_key_split, key_depth = jax.random.split(jax.random.fold_in(key, 13))
    extra_decay_rows = jax.random.randint(random_key_split, (2, HEAD_COUNT), 0, TOKEN_COUNT)
    cumulative_log_decay = jnp.log(jax.random.uniform(key_depth, (2, HEAD_COUNT), jnp.float32, 0.55, 0.8))
    position_index = jnp.arange(TOKEN_COUNT, dtype=jnp.int32)[:, None]
    summed_output = jnp.zeros((TOKEN_COUNT, HEAD_COUNT), jnp.float32)
    for block_total in range(2):
        summed_output = summed_output + jnp.where(position_index == extra_decay_rows[block_total][None, :], cumulative_log_decay[block_total][None, :], 0.0)
    return summed_output


def level_of(stream_key, extent, cuts, smallest, top_value):
    factor_of = 1.0
    for dim, shards_of in cuts:
        draws = jax.random.uniform(jax.random.fold_in(jax.random.fold_in(stream_key, 6), dim), (shards_of,), jnp.float32, smallest / len(cuts), top_value / len(cuts))
        factor_of = factor_of * jnp.repeat(jnp.exp(draws), extent[dim] // shards_of).reshape((-1,) + (1,) * (len(extent) - 1 - dim))
    return factor_of


def shared_out(key, own, number, rows, count, top, most, lean):
    order = jax.random.permutation(key, count)
    packed, common = load_shares(count, rows * top, most, lean, True), load_shares(count, rows * top, most, lean, False)
    places = jnp.arange(count)

    def named(sizes, turn):
        used = int((sizes > 0).sum())
        fixed = max(1, used // 4)
        passed = fixed + (places - fixed + turn * (used - fixed)) % max(1, count - fixed)
        return jnp.zeros((count,), jnp.int32).at[order[jnp.where(places < fixed, places, passed)]].set(jnp.asarray(sizes, jnp.int32))

    sizes = jnp.where(number % 4 == 0, named(packed, number // 4), named(common, number - number // 4 - 1))
    mixed = jax.random.permutation(jax.random.fold_in(own, 3), count)
    donor, receiver = mixed[0:count // 2 * 2:2], mixed[1:count // 2 * 2:2]
    room = jnp.minimum(sizes[donor] - 1, most - sizes[receiver]) // 2
    room = jnp.where((donor == order[0]) | (receiver == order[0]) | (sizes[receiver] == 0), 0, jnp.maximum(room, 0))
    passed = jax.random.randint(jax.random.fold_in(own, 4), (count // 2,), 0, 1 << 20) % (room + 1)
    sizes = sizes.at[donor].add(-passed).at[receiver].add(passed)
    items = jnp.searchsorted(jnp.cumsum(sizes), jnp.arange(rows * top), side="right").astype(jnp.int32)
    listing = items.reshape(top, rows).T
    listing = listing[jax.random.permutation(jax.random.fold_in(own, 1), rows)]
    turn = jax.random.randint(jax.random.fold_in(own, 2), (rows, 1), 0, top)
    return jnp.take_along_axis(listing, (jnp.arange(top)[None, :] + turn) % top, axis=1)


def load_shares(amount, total, reach, skew, full):
    weights = [(1 << 20) // math.isqrt(standing ** skew) + 1 for standing in range(1, amount + 1)]
    largest = reach if full else min(reach, max(-(-total // amount), total * weights[0] // sum(weights)))
    least = 1 if total - largest >= amount - 1 else 0
    counts, surplus = [largest] + [least] * (amount - 1), total - largest - least * (amount - 1)
    while surplus > 0:
        free = [i for i in range(1, amount) if counts[i] < largest] or [i for i in range(1, amount) if counts[i] < reach]
        pool, left = sum([weights[i] for i in free]), surplus
        for i in free:
            more = min(reach - counts[i], max(1, left * weights[i] // pool), surplus)
            counts[i] = counts[i] + more
            surplus = surplus - more
    return np.array(counts)


def noise(own_key, shape, scale, most, shards=(), kind=jnp.bfloat16):
    result = scale * jax.random.normal(own_key, shape, jnp.float32)
    if shards:
        result = result * level_of(own_key, shape, shards, -0.22, 0.18)
    return jnp.clip(result, -most, most).astype(kind)


def setup_inputs(seed: int = 0) -> dict:
    seeds = jax.random.split(jax.random.key(seed), 25)
    head_input_values = noise(seeds[0], (TOKEN_COUNT, INNER_WIDTH), 1.0, 6.0, ((0, 64), (1, 4)))
    group_input_vectors = noise(seeds[1], (TOKEN_COUNT, GROUP_COUNT * STATE_WIDTH), 1.0, 6.0, ((0, 64), (1, 4)))
    group_readout_vectors = noise(seeds[2], (TOKEN_COUNT, GROUP_COUNT * STATE_WIDTH), 1.0, 6.0, ((0, 64), (1, 4)))
    output_gate_values = noise(seeds[3], (TOKEN_COUNT, INNER_WIDTH), 1.0, 6.0, ((0, 64), (1, 4)))
    step_size_logits = draw_step_size_logits(jax.random.fold_in(seeds[24], 71), 0)
    extra_log_decay = draw_extra_log_decay(jax.random.fold_in(seeds[24], 71), 0)
    head_input_filter = noise(seeds[6], (TAPS, INNER_WIDTH), 0.5, 3.0, ((1, 4),))
    input_vector_filter = noise(seeds[7], (TAPS, GROUP_COUNT * STATE_WIDTH), 0.5, 3.0, ((1, 4),))
    readout_vector_filter = noise(seeds[8], (TAPS, GROUP_COUNT * STATE_WIDTH), 0.5, 3.0, ((1, 4),))
    step_size_bias = jnp.clip(jax.random.uniform(seeds[9], (HEAD_COUNT,), jnp.float32, -0.5, 0.5) * level_of(seeds[9], (HEAD_COUNT,), ((0, 4),), -0.4, 0.0), -0.5, 0.5)
    head_rate_logarithm = draw_head_rate_logarithm(jax.random.fold_in(seeds[24], 71), 0)
    direct_path_weight = jnp.clip(3.0 * jax.random.uniform(seeds[11], (HEAD_COUNT,), jnp.float32) ** level_of(seeds[11], (HEAD_COUNT,), ((0, 4),), -0.2, 0.2), 0.0, 3.0)
    group_norm_scale = jnp.clip(1.0 + 0.18 * jax.random.normal(seeds[12], (INNER_WIDTH,), jnp.float32), 0.099609375, 1.8984375).astype(jnp.bfloat16)
    mixer_output_weight = noise(seeds[13], (INNER_WIDTH, D), INNER_WIDTH ** -0.5, 0.09375, ((0, 4),))
    residual = noise(seeds[14], (TOKEN_COUNT, D), 1.0, 6.0, ((0, 256),))
    first_norm_scale = jnp.clip(1.0 + 0.18 * jax.random.normal(seeds[15], (D,), jnp.float32), 0.1, 1.9)
    first_norm_bias = noise(seeds[16], (D,), 0.3, 1.5, (), jnp.float32)
    routes_keys = jax.random.split(jax.random.fold_in(seeds[17], 1), TOKEN_COUNT // (TOK_DEV // N_TP))
    routes_turns = jax.random.permutation(jax.random.fold_in(seeds[17], 3), TOKEN_COUNT // (TOK_DEV // N_TP))
    routes = jax.vmap(lambda own, number: shared_out(jax.random.fold_in(seeds[17], 2), own, number, TOK_DEV // N_TP, EXPERTS, TOPK, CAP, 2))(routes_keys, routes_turns).reshape((TOKEN_COUNT, TOPK))
    routing_weight = jnp.clip(0.1 + 0.79999997 * jax.random.uniform(seeds[18], (TOKEN_COUNT, TOPK), jnp.float32) ** level_of(seeds[18], (TOKEN_COUNT, TOPK), ((0, 256),), -0.2, 0.2), 0.1, 0.9)
    expert_gate_weight = noise(seeds[19], (EXPERTS, D, FFE), D ** -0.5, 0.125, ((0, 64), (2, 4)))
    expert_up_weight = noise(seeds[20], (EXPERTS, D, FFE), D ** -0.5, 0.125, ((0, 64), (2, 4)))
    expert_down_weight = noise(seeds[21], (EXPERTS, D, FFE), FFE ** -0.5, 0.1875, ((0, 64), (2, 4)))
    final_norm_scale = jnp.clip(1.0 + 0.18 * jax.random.normal(seeds[22], (D,), jnp.float32), 0.1, 1.9)
    final_norm_bias = noise(seeds[23], (D,), 0.3, 1.5, (), jnp.float32)
    return dict(head_input_values=head_input_values, group_input_vectors=group_input_vectors, group_readout_vectors=group_readout_vectors, output_gate_values=output_gate_values, step_size_logits=step_size_logits, extra_log_decay=extra_log_decay, head_input_filter=head_input_filter, input_vector_filter=input_vector_filter, readout_vector_filter=readout_vector_filter, step_size_bias=step_size_bias, head_rate_logarithm=head_rate_logarithm, direct_path_weight=direct_path_weight, group_norm_scale=group_norm_scale, mixer_output_weight=mixer_output_weight, residual=residual, first_norm_scale=first_norm_scale, first_norm_bias=first_norm_bias, routes=routes, routing_weight=routing_weight, expert_gate_weight=expert_gate_weight, expert_up_weight=expert_up_weight, expert_down_weight=expert_down_weight, final_norm_scale=final_norm_scale, final_norm_bias=final_norm_bias)


EPS = 1e-05
ALPHA = 8.0 ** 0.25

def layer_norm(values, gain_row, bias_row):
    mean_value = lax.optimization_barrier(jnp.mean(values, axis=-1, keepdims=True))
    centred = values - mean_value
    spread = lax.optimization_barrier(jnp.mean(centred * centred, axis=-1, keepdims=True))
    return centred * lax.rsqrt(spread + EPS) * gain_row + bias_row

def conv_silu(raw_rows, tail_rows, tap_weights):
    full_rows = jnp.concatenate([tail_rows, raw_rows], axis=0).astype(jnp.float32)
    weights = tap_weights.astype(jnp.float32)
    length = raw_rows.shape[0]
    summed_output = jnp.zeros((length, raw_rows.shape[1]), jnp.float32)
    for offset in range(tap_weights.shape[0]):
        summed_output = summed_output + weights[offset] * full_rows[offset:offset + length]
    return jax.nn.silu(summed_output)

def block_pass(state_now, input_blocks):
    step_scaled_inputs, decay_logarithm, inputs_b, reads_c = input_blocks
    running = jnp.cumsum(decay_logarithm, axis=0)
    running_t = jnp.moveaxis(running, 0, -1)
    length = decay_logarithm.shape[0]
    causal = jnp.arange(length)[:, None] >= jnp.arange(length)[None, :]
    spread_log = jnp.where(causal, running_t[..., :, None] - running_t[..., None, :], -jnp.inf)
    decay_factors = jnp.exp(spread_log)
    decay_products = jnp.einsum('tgn,sgn->gts', reads_c, inputs_b, precision=lax.Precision.HIGHEST)
    within_block_output = jnp.einsum('zmka,azmo->kzmo', decay_products[:, None] * decay_factors, step_scaled_inputs, precision=lax.Precision.HIGHEST)
    carried_in = jnp.einsum('tgn,grpn->tgrp', reads_c, state_now, precision=lax.Precision.HIGHEST) * jnp.exp(running)[..., None]
    to_end = jnp.exp(running_t[..., -1:] - running_t)
    added = jnp.einsum('sgn,grs,sgrp->grpn', inputs_b, to_end, step_scaled_inputs, precision=lax.Precision.HIGHEST)
    state_next = jnp.exp(running_t[..., -1])[..., None, None] * state_now + added
    return (state_next, within_block_output + carried_in)

def slot_layout(block_routes, capacity, experts):
    flat_routes = block_routes.reshape(-1)
    matches = (flat_routes[:, None] == jnp.arange(experts, dtype=jnp.int32)[None, :]).astype(jnp.int32)
    before = jnp.cumsum(matches, axis=0) - matches
    return flat_routes * capacity + lax.optimization_barrier(jnp.sum(before * matches, axis=1))

def partial_layout(capacity, experts):

    def layout_one(block_routes):
        return slot_layout(block_routes, capacity, experts)
    return layout_one

def reference(head_input_values, group_input_vectors, group_readout_vectors, output_gate_values, step_size_logits, extra_log_decay, head_input_filter, input_vector_filter, readout_vector_filter, step_size_bias, head_rate_logarithm, direct_path_weight, group_norm_scale, mixer_output_weight, residual, first_norm_scale, first_norm_bias, routes, routing_weight, expert_gate_weight, expert_up_weight, expert_down_weight, final_norm_scale, final_norm_bias):
    repeat_count = HEAD_COUNT // GROUP_COUNT
    margin = TAPS - 1

    def mixer_block(carry, input_blocks):
        state_now, tail_x, tail_b, tail_c = carry
        unmixed_head_inputs, unmixed_input_vectors, unmixed_readout_vectors, unmixed_gate_values, unmixed_step_sizes, extra_decay_rows = input_blocks
        length = unmixed_head_inputs.shape[0]
        conv_x = conv_silu(unmixed_head_inputs, tail_x, head_input_filter)
        conv_b = conv_silu(unmixed_input_vectors, tail_b, input_vector_filter)
        conv_c = conv_silu(unmixed_readout_vectors, tail_c, readout_vector_filter)
        step_sizes = jax.nn.softplus(unmixed_step_sizes + step_size_bias)
        decay_logarithm = -step_sizes * jnp.exp(head_rate_logarithm) + extra_decay_rows
        heads_x = conv_x.reshape(length, GROUP_COUNT, repeat_count, HEAD_DIM)
        step_scaled_inputs = heads_x * step_sizes.reshape(length, GROUP_COUNT, repeat_count)[..., None]
        state_next, ssm_out = block_pass(state_now, (step_scaled_inputs, decay_logarithm.reshape(length, GROUP_COUNT, repeat_count), conv_b.reshape(length, GROUP_COUNT, STATE_WIDTH), conv_c.reshape(length, GROUP_COUNT, STATE_WIDTH)))
        ssm_out = ssm_out + direct_path_weight.reshape(GROUP_COUNT, repeat_count)[None, :, :, None] * heads_x
        gated = ssm_out.reshape(length, INNER_WIDTH) * jax.nn.silu(unmixed_gate_values.astype(jnp.float32))
        grouped = gated.reshape(length, GROUP_COUNT, -1)
        normed = grouped * lax.rsqrt(lax.optimization_barrier(jnp.mean(grouped * grouped, axis=-1, keepdims=True)) + EPS)
        rows_out = (normed.reshape(length, INNER_WIDTH) * group_norm_scale.astype(jnp.float32)).astype(jnp.bfloat16)
        return ((state_next, unmixed_head_inputs[length - margin:], unmixed_input_vectors[length - margin:], unmixed_readout_vectors[length - margin:]), rows_out)
    block_list = TOKEN_COUNT // BLOCK_LENGTH
    start = (jnp.zeros((GROUP_COUNT, repeat_count, HEAD_DIM, STATE_WIDTH), jnp.float32), jnp.zeros((margin, INNER_WIDTH), jnp.bfloat16), jnp.zeros((margin, GROUP_COUNT * STATE_WIDTH), jnp.bfloat16), jnp.zeros((margin, GROUP_COUNT * STATE_WIDTH), jnp.bfloat16))
    scan_results = (head_input_values.reshape(block_list, BLOCK_LENGTH, INNER_WIDTH), group_input_vectors.reshape(block_list, BLOCK_LENGTH, GROUP_COUNT * STATE_WIDTH), group_readout_vectors.reshape(block_list, BLOCK_LENGTH, GROUP_COUNT * STATE_WIDTH), output_gate_values.reshape(block_list, BLOCK_LENGTH, INNER_WIDTH), step_size_logits.reshape(block_list, BLOCK_LENGTH, HEAD_COUNT), extra_log_decay.reshape(block_list, BLOCK_LENGTH, HEAD_COUNT))
    unused_carry, mixer_rows = lax.scan(mixer_block, start, scan_results)
    mixer_rows = mixer_rows.reshape(TOKEN_COUNT, INNER_WIDTH)
    slice_width = INNER_WIDTH // N_TP
    mixed = jnp.zeros((TOKEN_COUNT, D), jnp.float32)
    for slice_index in range(N_TP):
        partial_value = jnp.dot(mixer_rows[:, slice_index * slice_width:(slice_index + 1) * slice_width], mixer_output_weight[slice_index * slice_width:(slice_index + 1) * slice_width], preferred_element_type=jnp.float32)
        rounded = lax.optimization_barrier(partial_value.astype(jnp.bfloat16))
        mixed = mixed + rounded.astype(jnp.float32)
    middle = layer_norm(ALPHA * residual.astype(jnp.float32) + mixed, first_norm_scale, first_norm_bias).astype(jnp.bfloat16)
    blocks_count = N_SP * N_TP
    rows_block = TOK_DEV // N_TP
    slot_ids = jax.vmap(partial_layout(CAP, EXPERTS))(routes.reshape(blocks_count, rows_block, TOPK))

    def fill_slots(block_rows, block_slots):
        owners = jnp.repeat(jnp.arange(rows_block, dtype=jnp.int32), TOPK)
        source = jnp.full((EXPERTS * CAP,), rows_block, jnp.int32).at[block_slots].set(owners)
        padded = jnp.concatenate([block_rows, jnp.zeros((1, D), jnp.bfloat16)], axis=0)
        return padded[source]
    buffers = jax.vmap(fill_slots)(middle.reshape(blocks_count, rows_block, D), slot_ids)
    buffers = buffers.reshape(blocks_count, EXPERTS, CAP, D)

    def one_expert(expert_index):
        rows_in = lax.dynamic_index_in_dim(buffers, expert_index, 1, keepdims=False).reshape(-1, D)
        weight_gate = lax.dynamic_index_in_dim(expert_gate_weight, expert_index, 0, keepdims=False)
        weight_up = lax.dynamic_index_in_dim(expert_up_weight, expert_index, 0, keepdims=False)
        weight_down = lax.dynamic_index_in_dim(expert_down_weight, expert_index, 0, keepdims=False)
        hidden = (jax.nn.silu(jnp.dot(rows_in, weight_gate, preferred_element_type=jnp.float32)) * jnp.dot(rows_in, weight_up, preferred_element_type=jnp.float32)).astype(jnp.bfloat16)
        return jnp.dot(hidden, weight_down.T, preferred_element_type=jnp.float32).astype(jnp.bfloat16)
    answers = lax.map(one_expert, jnp.arange(EXPERTS, dtype=jnp.int32))
    answers = answers.reshape(EXPERTS, blocks_count, CAP, D).transpose(1, 0, 2, 3).reshape(blocks_count, EXPERTS * CAP, D)

    def take_rows(block_answers, block_slots):
        return block_answers[block_slots]
    picked = jax.vmap(take_rows)(answers, slot_ids).astype(jnp.float32).reshape(TOKEN_COUNT, TOPK, D)
    ffn = lax.optimization_barrier(jnp.sum(picked * routing_weight[..., None], axis=1))
    return layer_norm(ALPHA * middle.astype(jnp.float32) + ffn, final_norm_scale, final_norm_bias).astype(jnp.bfloat16)
```

```python
import functools

import jax
import jax.numpy as jnp
from jax import lax
from jax.experimental import pallas as pl
from jax.experimental.pallas import tpu as pltpu
from jax.sharding import PartitionSpec as P

HEAD_DIM = 64
STATE_WIDTH = 128
BLOCK_LENGTH = 128
EPS = 1e-05
ALPHA = 8.0**0.25
LANES = 128
CAP = 5
Y_CORES = 8
PLANES = 8

f32 = jnp.float32
bf16 = jnp.bfloat16
MESH = pl.DeviceIdType.MESH
VMEM = pl.BlockSpec(memory_space=pltpu.VMEM)
SMEM = pl.BlockSpec(memory_space=pltpu.SMEM)
HBM = pl.BlockSpec(memory_space=pltpu.MemorySpace.HBM)


def silu(v):
    return v * (1.0 / (1.0 + jnp.exp(-v)))


def pair_wide(values, pair):
    rows = values.shape[0]
    lane = lax.broadcasted_iota(jnp.int32, (rows, LANES), 1)
    a = jnp.broadcast_to(values[:, 2 * pair : 2 * pair + 1], (rows, LANES))
    b = jnp.broadcast_to(values[:, 2 * pair + 1 : 2 * pair + 2], (rows, LANES))
    return jnp.where(lane < HEAD_DIM, a, b)


def norm_rows(values, gain, bias):
    centred = values - jnp.mean(values, axis=-1, keepdims=True)
    spread = jnp.mean(centred * centred, axis=-1, keepdims=True)
    return centred * lax.rsqrt(spread + EPS) * gain + bias


def plane_of(i):
    return jnp.where(lax.rem(i, 2) == 1, 4 - (i + 1) // 2, 4 + i // 2)


def layer_kernel(
    x_hbm, b_hbm, c_hbm, gate_hbm, logit_ref, extra_ref, fx_ref, fb_ref, fc_ref,
    bias_ref, rate_ref, direct_ref, gain_ref, wout_hbm, res_hbm, g1_ref, b1_ref,
    src_ref, slot_ref, rw_ref, wg_hbm, wu_hbm, wd_hbm, g2_ref, b2_ref,
    o_ref,
    x_scr, b_scr, c_scr, gate_scr, wout_scr, res_scr,
    tailx, tailb, tailc, pad_scr, y_scr, u_scr, bb_scr, cc_scr, run_scr, st_scr, gs_scr,
    logs_out, logs_in, pack, xin, eout, ein,
    part_scr, rs_in, mid3, tmpf, out5, rin, xrow, hid, ansb, fin, wbuf,
    lsem, wlsem, tail_s, tail_r, log_s, log_r, ex_s, ex_r, en_s, en_r, rs_s, rs_r, w_s, w_r, d_s, d_r, f_s, f_r,
):
    n_sp, n_tp = 64, 4
    s = lax.axis_index("sp")
    x = lax.axis_index("tp")
    z = s // Y_CORES
    yc = lax.rem(s, Y_CORES)
    core = lax.rem(s, 2)
    odd = lax.rem(x, 2)
    xp = jnp.where(odd == 1, lax.rem(x + 1, n_tp), lax.rem(x + n_tp - 1, n_tp))
    is_root = core == odd
    length, width = x_scr.shape
    gw = b_scr.shape[1]
    taps = fx_ref.shape[0]
    heads = logit_ref.shape[1]
    groups = gw // STATE_WIDTH
    per = width // groups
    pairs = per // LANES
    panels = width // LANES
    L = BLOCK_LENGTH
    blocks = length // L
    rows_here, model = o_ref.shape
    chunks = model // LANES

    def remote(src, dst, ss, rr, dev):
        return pltpu.make_async_remote_copy(
            src_ref=src, dst_ref=dst, send_sem=ss, recv_sem=rr, device_id=dev, device_id_type=MESH
        )

    here = [
        pltpu.make_async_copy(a, b, lsem.at[i])
        for i, (a, b) in enumerate(
            ((x_hbm, x_scr), (b_hbm, b_scr), (c_hbm, c_scr), (gate_hbm, gate_scr), (wout_hbm, wout_scr), (res_hbm, res_scr))
        )
    ]
    for copy in here:
        copy.start()
    experts_w = (wg_hbm, wu_hbm, wd_hbm)

    @pl.when(is_root)
    def _():
        for m in range(3):
            pltpu.make_async_copy(experts_w[m].at[0], wbuf.at[m, x], wlsem.at[m]).start()

    barrier = pltpu.get_barrier_semaphore()

    def greet(d, carry):
        t = lax.rem(s + d, n_sp)
        pl.semaphore_signal(barrier, inc=1, device_id=(t, x), device_id_type=MESH)

        @pl.when(jnp.logical_or(is_root, lax.rem(t, 2) == 1 - odd))
        def _():
            pl.semaphore_signal(barrier, inc=1, device_id=(t, xp), device_id_type=MESH)

        return carry

    lax.fori_loop(1, n_sp, greet, 0)
    for d in range(1, n_tp):
        pl.semaphore_signal(barrier, inc=1, device_id=(s, lax.rem(x + d, n_tp)), device_id_type=MESH)

    v = logit_ref[...] + bias_ref[...]
    step = jnp.maximum(v, 0.0) + jnp.log(1.0 + jnp.exp(-jnp.abs(v)))
    decay = -step * jnp.exp(rate_ref[...]) + extra_ref[...]
    ti = lax.broadcasted_iota(jnp.int32, (L, L), 0)
    si = lax.broadcasted_iota(jnp.int32, (L, L), 1)
    causal = ti >= si
    tri = causal.astype(f32)
    runs = []
    before = jnp.zeros((1, heads), f32)
    for k in range(blocks):
        r = jnp.dot(tri, decay[k * L : (k + 1) * L], precision=lax.Precision.HIGHEST, preferred_element_type=f32)
        runs.append(r)
        run_scr[k * L : (k + 1) * L, :] = r + before
        before = before + r[L - 1 : L]
    for p in range(panels):
        logs_out[p] = pair_wide(before, p)
    here[3].wait()

    def gate_rows(i, carry):
        rows = pl.ds(pl.multiple_of(i * 32, 32), 32)
        gs_scr[rows, :] = silu(gate_scr[rows, :].astype(f32))
        return carry

    lax.fori_loop(0, length // 32, gate_rows, 0)
    for copy in here[:3]:
        copy.wait()

    pl.semaphore_wait(barrier, n_sp - 1 + n_tp - 1 + jnp.where(is_root, n_sp - 1, n_sp // 2 - 1))

    tails = (
        (x_scr, tailx, 0), (b_scr, tailb, 1), (c_scr, tailc, 2),
    )

    def tail_copy(a, t, i, target):
        return remote(a.at[pl.ds(length - 8, 8)], t, tail_s.at[i], tail_r.at[i], (target, x))

    @pl.when(s < n_sp - 1)
    def _():
        for a, t, i in tails:
            tail_copy(a, t, i, s + 1).start()

    def send_log(d, carry):
        t = lax.rem(s + d, n_sp)
        remote(logs_out.at[lax.rem(t, panels)], logs_in.at[s], log_s, log_r, (t, x)).start()
        return carry

    lax.fori_loop(1, n_sp, send_log, 0)
    logs_in[s] = logs_out[lax.rem(s, panels)]

    def weight_copy(m, k, target):
        return remote(experts_w[m].at[0], wbuf.at[m, x], w_s.at[m, k], w_r.at[m], (s, target))

    @pl.when(is_root)
    def _():
        for m in range(3):
            weight_copy(m, 0, lax.rem(x + 2, n_tp)).start()

    @pl.when(jnp.logical_not(is_root))
    def _():
        for m in range(3):
            weight_copy(m, 0, lax.rem(x + 1, n_tp)).start()
            weight_copy(m, 1, lax.rem(x + 3, n_tp)).start()

    @pl.when(s == 0)
    def _():
        for _, t, _i in tails:
            t[...] = jnp.zeros_like(t)

    @pl.when(s > 0)
    def _():
        for a, t, i in tails:
            tail_copy(a, t, i, s - 1).wait_recv()

    def conv(raw_ref, tail_ref, filt_ref, col):
        pad_scr[0:8, :] = tail_ref[:, col : col + LANES].astype(f32)
        pad_scr[8 : 8 + length, :] = raw_ref[:, col : col + LANES].astype(f32)
        acc = None
        for o in range(taps):
            start = 8 - (taps - 1) + o
            part = pad_scr[start : start + length, :] * filt_ref[o : o + 1, col : col + LANES].astype(f32)
            acc = part if acc is None else acc + part
        return silu(acc)

    for g in range(groups):
        col = g * STATE_WIDTH
        bb_scr[:, col : col + LANES] = conv(b_scr, tailb, fb_ref, col).astype(bf16)
    for g in range(groups):
        ncol = g * STATE_WIDTH
        for p in range(pairs):
            q = g * pairs + p
            cols = slice(q * LANES, (q + 1) * LANES)
            xc = conv(x_scr, tailx, fx_ref, q * LANES)
            y_scr[:, cols] = xc * pair_wide(direct_ref[...], q)
            u_scr[:, cols] = (xc * pair_wide(step, q)).astype(bf16)
            state = None
            for k in range(blocks):
                rows = slice(k * L, (k + 1) * L)
                run = runs[k]
                end = run[L - 1 : L]
                leave = pair_wide(jnp.exp(end - run), q)
                added = lax.dot_general(
                    bb_scr[rows, ncol : ncol + LANES],
                    (u_scr[rows, cols].astype(f32) * leave).astype(bf16),
                    (((0,), (0,)), ((), ())), preferred_element_type=f32,
                )
                state = added if k == 0 else state * pair_wide(jnp.exp(end), q) + added
                if k < blocks - 1:
                    st_scr[k, :, cols] = state.astype(bf16)
            state = state.astype(bf16)
            for r in range(STATE_WIDTH // 16):
                pack[r * panels + q] = state[r * 16 : (r + 1) * 16]

    def send_state(d, carry):
        t = lax.rem(s + d, n_sp)
        remote(pack.at[t], xin.at[s], ex_s, ex_r, (t, x)).start()
        return carry

    lax.fori_loop(1, n_sp, send_state, 0)
    xin[s] = pack[s]

    for g in range(groups):
        col = g * STATE_WIDTH
        cc_scr[:, col : col + LANES] = conv(c_scr, tailc, fc_ref, col).astype(bf16)
    lane = lax.broadcasted_iota(jnp.int32, (L, LANES), 1)
    for g in range(groups):
        ncol = g * STATE_WIDTH
        for k in range(blocks):
            rows = slice(k * L, (k + 1) * L)
            cb = cc_scr[rows, ncol : ncol + LANES]
            bb = bb_scr[rows, ncol : ncol + LANES]
            prod = lax.dot_general(cb, bb, (((1,), (1,)), ((), ())), preferred_element_type=f32)
            run = runs[k]
            run_t = run.T
            enter = jnp.exp(run)
            for p in range(pairs):
                q = g * pairs + p
                cols = slice(q * LANES, (q + 1) * LANES)
                u = u_scr[rows, cols]
                mats = []
                for h in (2 * q, 2 * q + 1):
                    diff = jnp.where(causal, run[:, h : h + 1] - run_t[h : h + 1, :], -1e30)
                    mats.append((prod * jnp.exp(diff)).astype(bf16))
                zero = jnp.zeros_like(u)
                both = jnp.concatenate(
                    [jnp.where(lane < HEAD_DIM, u, zero), jnp.where(lane < HEAD_DIM, zero, u)], axis=0
                )
                out = jnp.dot(jnp.concatenate(mats, axis=1), both, preferred_element_type=f32)
                if k > 0:
                    out = out + pair_wide(enter, q) * jnp.dot(
                        cb, st_scr[k - 1, :, cols], preferred_element_type=f32
                    )
                y_scr[rows, cols] = y_scr[rows, cols] + out

    def got(ref, ss, rr):
        return remote(ref, ref, ss, rr, (lax.rem(s + 1, n_sp), x))

    got(logs_in.at[pl.ds(0, n_sp - 1)], log_s, log_r).wait_recv()
    got(xin.at[pl.ds(0, n_sp - 1)], ex_s, ex_r).wait_recv()
    factors = jnp.exp(logs_in[...].reshape(n_sp, LANES))
    logs_in[...] = factors.reshape(n_sp, 1, LANES)

    def turn(i, now):
        eout[i] = now.astype(bf16)
        return logs_in[i] * now + xin[i].astype(f32)

    lax.fori_loop(0, n_sp, turn, jnp.zeros((16, LANES), f32), unroll=8)

    def send_enter(d, carry):
        t = lax.rem(s + d, n_sp)
        remote(eout.at[t], ein.at[s], en_s, en_r, (t, x)).start()
        return carry

    lax.fori_loop(1, n_sp, send_enter, 0)
    ein[s] = eout[s]
    here[4].wait()
    here[5].wait()
    got(ein.at[pl.ds(0, n_sp - 1)], en_s, en_r).wait_recv()

    enters = [
        jnp.concatenate([ein[r * panels + q] for r in range(STATE_WIDTH // 16)], axis=0) for q in range(panels)
    ]

    def rs_copy(d):
        return remote(part_scr.at[d], rs_in.at[d], rs_s.at[d], rs_r.at[d], (s, lax.rem(x + d, n_tp)))

    def mix_rows(i, carry):
        d = jnp.where(i == 0, 2, jnp.where(i == 1, 1, jnp.where(i == 2, 3, 0)))
        rows = pl.ds(pl.multiple_of(lax.rem(x + d, n_tp) * rows_here, 32), rows_here)
        enter = jnp.exp(run_scr[rows, :])
        normed = []
        for g in range(groups):
            cb = cc_scr[rows, g * STATE_WIDTH : (g + 1) * STATE_WIDTH]
            cols = slice(g * per, (g + 1) * per)
            read = jnp.concatenate(
                [
                    jnp.dot(cb, enters[g * pairs + p], preferred_element_type=f32) * pair_wide(enter, g * pairs + p)
                    for p in range(pairs)
                ],
                axis=1,
            )
            gated = (y_scr[rows, cols] + read) * gs_scr[rows, cols]
            scale = lax.rsqrt(jnp.mean(gated * gated, axis=-1, keepdims=True) + EPS)
            normed.append((gated * scale * gain_ref[:, cols].astype(f32)).astype(bf16))
        part_scr[d] = jnp.dot(
            jnp.concatenate(normed, axis=1), wout_scr[...], preferred_element_type=f32
        ).astype(bf16)

        @pl.when(d != 0)
        def _():
            rs_copy(d).start()

        return carry

    lax.fori_loop(0, n_tp, mix_rows, 0)
    mixed = part_scr[0].astype(f32)
    for d in (1, 3, 2):
        rs_copy(d).wait_recv()
        mixed = mixed + rs_in[d].astype(f32)
    middle = norm_rows(ALPHA * res_scr[...].astype(f32) + mixed, g1_ref[...], b1_ref[...]).astype(bf16).astype(f32)
    for c in range(chunks):
        tmpf[pl.ds(c, rows_here, stride=chunks), :] = middle[:, c * LANES : (c + 1) * LANES]
    mid3[...] = tmpf[0 : rows_here * chunks, :].reshape(rows_here, chunks, LANES).astype(bf16)

    def send_plane(i, carry):
        zt = lax.rem(z + plane_of(i), PLANES)

        def send_one(j, carry):
            t = zt * Y_CORES + lax.rem(yc + j, Y_CORES)
            for k in range(CAP):
                out5[t, k] = mid3[src_ref[t * CAP + k]]
            same = lax.rem(t, 2) == odd
            slot = (i * 2 + jnp.where(same, 0, 1)) * Y_CORES + yc
            mine = jnp.logical_and(t == s, same)

            @pl.when(mine)
            def _():
                rin[slot] = out5[t]

            @pl.when(jnp.logical_not(mine))
            def _():
                remote(out5.at[t], rin.at[slot], d_s, d_r.at[i // 2], (t, jnp.where(same, x, xp))).start()

            return carry

        lax.fori_loop(0, Y_CORES, send_one, 0)
        return carry

    lax.fori_loop(0, PLANES, send_plane, 0)

    quarter = 4 * Y_CORES

    @pl.when(is_root)
    def _():
        for m in range(3):
            pltpu.make_async_copy(experts_w[m].at[0], wbuf.at[m, x], wlsem.at[m]).wait()
            ref = wbuf.at[m, pl.ds(0, n_tp - 1)]
            remote(ref, ref, w_s.at[m, 0], w_r.at[m], (lax.rem(s + 1, n_sp), x)).wait_recv()

        def expert_chunk(ci, carry):
            base = ci * quarter

            @pl.when(ci < 3)
            def _():
                got(rin.at[pl.ds(0, quarter)], d_s, d_r.at[ci]).wait_recv()

            @pl.when(ci == 3)
            def _():
                got(rin.at[pl.ds(0, quarter - 1)], d_s, d_r.at[ci]).wait_recv()

            n = quarter * CAP
            tmpf[...] = rin[pl.ds(base, quarter)].astype(f32).reshape(n * chunks, LANES)
            for c in range(chunks):
                xrow[:, c * LANES : (c + 1) * LANES] = tmpf[pl.ds(c, n, stride=chunks), :].astype(bf16)
            for t in range(n_tp):
                gate = jnp.dot(xrow[...], wbuf[0, t], preferred_element_type=f32)
                up = jnp.dot(xrow[...], wbuf[1, t], preferred_element_type=f32)
                hid[t] = (silu(gate) * up).astype(bf16)
            for o in range(chunks // 2):
                ans = None
                for t in range(n_tp):
                    part = lax.dot_general(
                        hid[t], wbuf[2, t, 2 * o * LANES : 2 * (o + 1) * LANES, :],
                        (((1,), (1,)), ((), ())), preferred_element_type=f32,
                    )
                    ans = part if ans is None else ans + part
                tmpf[pl.ds(2 * o, n, stride=chunks), :] = ans[:, :LANES]
                tmpf[pl.ds(2 * o + 1, n, stride=chunks), :] = ans[:, LANES:]
            ansb[pl.ds(base, quarter)] = tmpf[...].reshape(quarter, CAP, chunks, LANES).astype(bf16)

            def send_back(m, carry):
                slot = base + m
                i = slot // 16
                same = lax.rem(slot // 8, 2) == 0
                t = lax.rem(z + PLANES - plane_of(i), PLANES) * Y_CORES + lax.rem(slot, 8)
                mine = jnp.logical_and(t == s, same)

                @pl.when(mine)
                def _():
                    fin[s] = ansb[slot]

                @pl.when(jnp.logical_not(mine))
                def _():
                    remote(ansb.at[slot], fin.at[s], f_s, f_r, (t, jnp.where(same, x, xp))).start()

                return carry

            lax.fori_loop(0, quarter, send_back, 0)
            return carry

        lax.fori_loop(0, 4, expert_chunk, 0)
        got(fin.at[pl.ds(0, n_sp - 1)], f_s, f_r).wait_recv()

    @pl.when(jnp.logical_not(is_root))
    def _():
        got(fin.at[pl.ds(0, n_sp)], f_s, f_r).wait_recv()

    def combine(r, carry):
        total = ALPHA * mid3[r].astype(f32)
        ffn = None
        for k in range(2):
            slot = slot_ref[2 * r + k]
            part = fin[slot // CAP, lax.rem(slot, CAP)].astype(f32) * rw_ref[2 * r + k]
            ffn = part if ffn is None else ffn + part
        tmpf[pl.ds(pl.multiple_of(r * chunks, chunks), chunks), :] = total + ffn
        return carry

    lax.fori_loop(0, rows_here, combine, 0, unroll=4)
    total = jnp.concatenate([tmpf[pl.ds(c, rows_here, stride=chunks), :] for c in range(chunks)], axis=1)
    o_ref[...] = norm_rows(total, g2_ref[...], b2_ref[...]).astype(bf16)

    @pl.when(s < n_sp - 1)
    def _():
        for a, t, i in tails:
            tail_copy(a, t, i, s + 1).wait_send()

    got(logs_in.at[pl.ds(0, n_sp - 1)], log_s, log_r).wait_send()
    got(xin.at[pl.ds(0, n_sp - 1)], ex_s, ex_r).wait_send()
    got(ein.at[pl.ds(0, n_sp - 1)], en_s, en_r).wait_send()
    for d in range(1, n_tp):
        rs_copy(d).wait_send()

    @pl.when(is_root)
    def _():
        for m in range(3):
            weight_copy(m, 0, lax.rem(x + 2, n_tp)).wait_send()
        got(out5.at[pl.ds(0, n_sp - 1)], d_s, d_r.at[0]).wait_send()
        got(ansb.at[pl.ds(0, 2 * n_sp - 1)], f_s, f_r).wait_send()

    @pl.when(jnp.logical_not(is_root))
    def _():
        for m in range(3):
            weight_copy(m, 0, lax.rem(x + 1, n_tp)).wait_send()
            weight_copy(m, 1, lax.rem(x + 3, n_tp)).wait_send()
        got(out5.at[pl.ds(0, n_sp)], d_s, d_r.at[0]).wait_send()


def slot_layout(block_routes, capacity, experts):
    flat_routes = block_routes.reshape(-1)
    n = flat_routes.shape[0]
    earlier = jnp.arange(n)[:, None] > jnp.arange(n)[None, :]
    same = flat_routes[:, None] == flat_routes[None, :]
    rank = jnp.sum((earlier & same).astype(jnp.int32), axis=1)
    slots = flat_routes * capacity + rank
    hit = slots[:, None] == jnp.arange(experts * capacity, dtype=jnp.int32)[None, :]
    source = jnp.sum(jnp.where(hit, (jnp.arange(n, dtype=jnp.int32) // block_routes.shape[1])[:, None], 0), axis=0)
    return slots, source


def shards(
    head_input_values, group_input_vectors, group_readout_vectors, output_gate_values,
    step_size_logits, extra_log_decay, head_input_filter, input_vector_filter,
    readout_vector_filter, step_size_bias, head_rate_logarithm, direct_path_weight,
    group_norm_scale, mixer_output_weight, residual, first_norm_scale, first_norm_bias,
    routes, routing_weight, expert_gate_weight, expert_up_weight, expert_down_weight,
    final_norm_scale, final_norm_bias,
):
    n_sp, n_tp = lax.axis_size("sp"), lax.axis_size("tp")
    length, width = head_input_values.shape
    gw = group_input_vectors.shape[1]
    heads = step_size_logits.shape[1]
    rows_here, model = residual.shape
    hidden = expert_gate_weight.shape[2]
    chunks = model // LANES
    panels = width // LANES
    slots, source = slot_layout(routes, CAP, n_sp)
    dma = pltpu.SemaphoreType.DMA
    quarter_rows = 4 * Y_CORES * CAP
    return pl.pallas_call(
        layer_kernel,
        out_shape=jax.ShapeDtypeStruct((rows_here, model), bf16),
        in_specs=[HBM] * 4 + [VMEM] * 9 + [HBM] * 2 + [VMEM] * 2 + [SMEM] * 3 + [HBM] * 3 + [VMEM] * 2,
        out_specs=VMEM,
        scratch_shapes=[
            pltpu.VMEM((length, width), bf16),
            pltpu.VMEM((length, gw), bf16),
            pltpu.VMEM((length, gw), bf16),
            pltpu.VMEM((length, width), bf16),
            pltpu.VMEM((width, model), bf16),
            pltpu.VMEM((rows_here, model), bf16),
            pltpu.VMEM((8, width), bf16),
            pltpu.VMEM((8, gw), bf16),
            pltpu.VMEM((8, gw), bf16),
            pltpu.VMEM((length + 8, LANES), f32),
            pltpu.VMEM((length, width), f32),
            pltpu.VMEM((length, width), bf16),
            pltpu.VMEM((length, gw), bf16),
            pltpu.VMEM((length, gw), bf16),
            pltpu.VMEM((length, heads), f32),
            pltpu.VMEM((2, STATE_WIDTH, width), bf16),
            pltpu.VMEM((length, width), f32),
            pltpu.VMEM((panels, 1, LANES), f32),
            pltpu.VMEM((n_sp, 1, LANES), f32),
            pltpu.VMEM((n_sp, 16, LANES), bf16),
            pltpu.VMEM((n_sp, 16, LANES), bf16),
            pltpu.VMEM((n_sp, 16, LANES), bf16),
            pltpu.VMEM((n_sp, 16, LANES), bf16),
            pltpu.VMEM((n_tp, rows_here, model), bf16),
            pltpu.VMEM((n_tp, rows_here, model), bf16),
            pltpu.VMEM((rows_here, chunks, LANES), bf16),
            pltpu.VMEM((quarter_rows * chunks, LANES), f32),
            pltpu.VMEM((n_sp, CAP, chunks, LANES), bf16),
            pltpu.VMEM((2 * n_sp, CAP, chunks, LANES), bf16),
            pltpu.VMEM((quarter_rows, model), bf16),
            pltpu.VMEM((n_tp, quarter_rows, hidden), bf16),
            pltpu.VMEM((2 * n_sp, CAP, chunks, LANES), bf16),
            pltpu.VMEM((n_sp, CAP, chunks, LANES), bf16),
            pltpu.VMEM((3, n_tp, model, hidden), bf16),
            dma((6,)), dma((3,)), dma((3,)), dma((3,)), dma, dma, dma, dma, dma, dma,
            dma((n_tp,)), dma((n_tp,)), dma((3, 2)), dma((3,)), dma, dma((4,)), dma, dma,
        ],
        compiler_params=pltpu.CompilerParams(
            collective_id=0, has_side_effects=True, vmem_limit_bytes=60 * 1024 * 1024
        ),
        name="layer",
    )(
        head_input_values, group_input_vectors, group_readout_vectors, output_gate_values,
        step_size_logits, extra_log_decay, head_input_filter, input_vector_filter, readout_vector_filter,
        step_size_bias.reshape(1, heads), head_rate_logarithm.reshape(1, heads), direct_path_weight.reshape(1, heads),
        group_norm_scale.reshape(1, width), mixer_output_weight, residual,
        first_norm_scale.reshape(1, model), first_norm_bias.reshape(1, model),
        source, slots, routing_weight.reshape(-1),
        expert_gate_weight, expert_up_weight, expert_down_weight,
        final_norm_scale.reshape(1, model), final_norm_bias.reshape(1, model),
    )


def solution(mesh):
    in_specs = (
        P("sp", "tp"), P("sp", "tp"), P("sp", "tp"), P("sp", "tp"), P("sp", "tp"), P("sp", "tp"),
        P(None, "tp"), P(None, "tp"), P(None, "tp"), P("tp"), P("tp"), P("tp"), P("tp"),
        P("tp", None), P(("sp", "tp"), None), P(), P(), P(("sp", "tp"), None), P(("sp", "tp"), None),
        P("sp", None, "tp"), P("sp", None, "tp"), P("sp", None, "tp"), P(), P(),
    )
    out_specs = P(("sp", "tp"), None)
    return jax.shard_map(shards, mesh=mesh, in_specs=in_specs, out_specs=out_specs, check_vma=False)
```

```python
import functools

import jax
import jax.numpy as jnp
from jax import lax
from jax.experimental import pallas as pl
from jax.experimental.pallas import tpu as pltpu
from jax.sharding import PartitionSpec as P

HEAD_DIM = 64
STATE_WIDTH = 128
BLOCK_LENGTH = 128
EPS = 1e-05
ALPHA = 8.0**0.25
LANES = 128
CAP = 5
N_EXPERTS = 64
Y_CORES = 8
PLANES = 8

f32 = jnp.float32
bf16 = jnp.bfloat16
MESH = pl.DeviceIdType.MESH
VMEM = pl.BlockSpec(memory_space=pltpu.VMEM)
SMEM = pl.BlockSpec(memory_space=pltpu.SMEM)
HBM = pl.BlockSpec(memory_space=pltpu.MemorySpace.HBM)


def silu(v):
    return v * (1.0 / (1.0 + jnp.exp(-v)))


def pair_wide(values, pair):
    rows = values.shape[0]
    lane = lax.broadcasted_iota(jnp.int32, (rows, LANES), 1)
    a = jnp.broadcast_to(values[:, 2 * pair : 2 * pair + 1], (rows, LANES))
    b = jnp.broadcast_to(values[:, 2 * pair + 1 : 2 * pair + 2], (rows, LANES))
    return jnp.where(lane < HEAD_DIM, a, b)


def norm_rows(values, gain, bias):
    centred = values - jnp.mean(values, axis=-1, keepdims=True)
    spread = jnp.mean(centred * centred, axis=-1, keepdims=True)
    return centred * lax.rsqrt(spread + EPS) * gain + bias


SHIFTS = (3, 5, 4, 0, 2, 6, 1, 7)


def layer_kernel(
    x_hbm, b_hbm, c_hbm, gate_hbm, logit_ref, extra_ref, fx_ref, fb_ref, fc_ref,
    bias_ref, rate_ref, direct_ref, gain_ref, wout_hbm, res_hbm, g1_ref, b1_ref,
    src_ref, slot_ref, rw_ref, wg_hbm, wu_hbm, wd_hbm, g2_ref, b2_ref,
    o_ref,
    x_scr, b_scr, c_scr, gate_scr, wout_scr, res_scr,
    tailx, tailb, tailc, pad_scr, y_scr, u_scr, bb_scr, cc_scr, run_scr, st_scr, gs_scr,
    logs_out, logs_in, pack, xin, eout, ein,
    part_scr, relay, rs_in, mid3, tmpf, out5, rin, xrow, gated_scr, hid, ansb, fin, stage, wbuf,
    lsem, wlsem, tail_s, tail_r, log_s, log_r, ex_s, ex_r, en_s, en_r, rs_s, rs_r, w_s, w_r, d_s, d_r, f_s, f_r,
):
    n_sp, n_tp = 64, 4
    s = lax.axis_index("sp")
    x = lax.axis_index("tp")
    z = s // Y_CORES
    yc = lax.rem(s, Y_CORES)
    core = lax.rem(s, 2)
    odd = lax.rem(x, 2)
    right, left = lax.rem(x + 1, n_tp), lax.rem(x + n_tp - 1, n_tp)

    def beyond(plane):
        return jnp.where(lax.rem(plane, 2) == 0, right, left)

    xp = jnp.where(lax.rem(z, 2) == 0, left, right)
    is_root = core == odd
    length, width = x_scr.shape
    gw = b_scr.shape[1]
    taps = fx_ref.shape[0]
    heads = logit_ref.shape[0]
    groups = gw // STATE_WIDTH
    per = width // groups
    pairs = per // LANES
    panels = width // LANES
    L = BLOCK_LENGTH
    blocks = length // L
    rows_here, model = o_ref.shape
    chunks = model // LANES

    def remote(src, dst, ss, rr, dev):
        return pltpu.make_async_remote_copy(
            src_ref=src, dst_ref=dst, send_sem=ss, recv_sem=rr, device_id=dev, device_id_type=MESH
        )

    here = [
        pltpu.make_async_copy(a, b, lsem.at[i])
        for i, (a, b) in enumerate(
            ((x_hbm, x_scr), (b_hbm, b_scr), (c_hbm, c_scr), (gate_hbm, gate_scr), (wout_hbm, wout_scr), (res_hbm, res_scr))
        )
    ]
    for copy in here:
        copy.start()
    experts_w = (wg_hbm, wu_hbm, wd_hbm)
    half = model // 2

    def own_weight(m):
        return pltpu.make_async_copy(experts_w[m].at[0], wbuf.at[m, x], wlsem.at[m])

    @pl.when(is_root)
    def _():
        for m in range(3):
            own_weight(m).start()

    piece = model // 4
    pieces = [(0, 0, model, 0)] + [(1, q * piece, piece, 1) for q in range(4)] + [
        (2, q * piece, piece, 2 + q) for q in range(4)
    ]

    def send_weight(k):
        m, first, count, sem = pieces[k]
        rows = pl.ds(first, count)

        def send(target):
            remote(experts_w[m].at[0, rows], wbuf.at[m, x, rows], w_s.at[k], w_r.at[sem], (s, target)).start()

        @pl.when(is_root)
        def _():
            send(lax.rem(x + 2, n_tp))

        @pl.when(jnp.logical_not(is_root))
        def _():
            send(lax.rem(x + 1, n_tp))
            send(lax.rem(x + 3, n_tp))

    def sent_weight(k, root):
        m, first, count, sem = pieces[k]
        ref = wbuf.at[m, 0, pl.ds(first, count)] if root else wbuf.at[m, pl.ds(0, 2), pl.ds(first, count)]
        remote(ref, ref, w_s.at[k], w_r.at[sem], (lax.rem(s + 1, n_sp), x)).wait_send()

    barrier = pltpu.get_barrier_semaphore()

    def greet(d, carry):
        t = lax.rem(s + d, n_sp)
        pl.semaphore_signal(barrier, inc=1, device_id=(t, x), device_id_type=MESH)
        return carry

    lax.fori_loop(1, n_sp, greet, 0)

    def greet_experts(k, carry):
        t = 2 * k + 1 - odd
        pl.semaphore_signal(barrier, inc=1, device_id=(t, beyond(t // Y_CORES)), device_id_type=MESH)
        return carry

    lax.fori_loop(0, n_sp // 2, greet_experts, 0)

    @pl.when(is_root)
    def _():
        def greet_senders(t, carry):
            pl.semaphore_signal(barrier, inc=1, device_id=(t, xp), device_id_type=MESH)
            return carry

        lax.fori_loop(0, n_sp, greet_senders, 0)

    for d in range(1, n_tp):
        pl.semaphore_signal(barrier, inc=1, device_id=(s, lax.rem(x + d, n_tp)), device_id_type=MESH)

    v = logit_ref[...] + bias_ref[...].T
    step_t = jnp.maximum(v, 0.0) + jnp.log(1.0 + jnp.exp(-jnp.abs(v)))
    decay_t = -step_t * jnp.exp(rate_ref[...].T) + extra_ref[...]
    step = step_t.T
    ti = lax.broadcasted_iota(jnp.int32, (L, L), 0)
    si = lax.broadcasted_iota(jnp.int32, (L, L), 1)
    causal = ti >= si
    tri = (ti <= si).astype(f32)
    runs, runs_t = [], []
    before = jnp.zeros((1, heads), f32)
    for k in range(blocks):
        r_t = jnp.dot(decay_t[:, k * L : (k + 1) * L], tri, precision=lax.Precision.HIGHEST, preferred_element_type=f32)
        r = r_t.T
        runs_t.append(r_t)
        runs.append(r)
        run_scr[k * L : (k + 1) * L, :] = r + before
        before = before + r[L - 1 : L]
    for p in range(panels):
        logs_out[p] = pair_wide(before, p)
    here[3].wait()

    def gate_rows(i, carry):
        rows = pl.ds(pl.multiple_of(i * 32, 32), 32)
        gs_scr[rows, :] = silu(gate_scr[rows, :].astype(f32))
        return carry

    lax.fori_loop(0, length // 32, gate_rows, 0)
    for copy in here[:3]:
        copy.wait()

    pl.semaphore_wait(barrier, n_sp - 1 + n_tp - 1 + n_sp // 2 + jnp.where(is_root, n_sp, 0))

    tails = (
        (x_scr, tailx, 0), (b_scr, tailb, 1), (c_scr, tailc, 2),
    )

    def tail_copy(a, t, i, target):
        return remote(a.at[pl.ds(length - 8, 8)], t, tail_s.at[i], tail_r.at[i], (target, x))

    @pl.when(s < n_sp - 1)
    def _():
        for a, t, i in tails:
            tail_copy(a, t, i, s + 1).start()

    def send_log(d, carry):
        t = lax.rem(s + d, n_sp)
        remote(logs_out.at[lax.rem(t, panels)], logs_in.at[s], log_s, log_r, (t, x)).start()
        return carry

    lax.fori_loop(1, n_sp, send_log, 0)
    logs_in[s] = logs_out[lax.rem(s, panels)]

    send_weight(0)
    send_weight(1)

    @pl.when(s == 0)
    def _():
        for _, t, _i in tails:
            t[...] = jnp.zeros_like(t)

    @pl.when(s > 0)
    def _():
        for a, t, i in tails:
            tail_copy(a, t, i, s - 1).wait_recv()

    def conv(raw_ref, tail_ref, filt_ref, col):
        pad_scr[0:8, :] = tail_ref[:, col : col + LANES].astype(f32)
        pad_scr[8 : 8 + length, :] = raw_ref[:, col : col + LANES].astype(f32)
        acc = None
        for o in range(taps):
            start = 8 - (taps - 1) + o
            part = pad_scr[start : start + length, :] * filt_ref[o : o + 1, col : col + LANES].astype(f32)
            acc = part if acc is None else acc + part
        return silu(acc)

    for g in range(groups):
        col = g * STATE_WIDTH
        bb_scr[:, col : col + LANES] = conv(b_scr, tailb, fb_ref, col).astype(bf16)
    for g in range(groups):
        ncol = g * STATE_WIDTH
        for p in range(pairs):
            q = g * pairs + p
            cols = slice(q * LANES, (q + 1) * LANES)
            xc = conv(x_scr, tailx, fx_ref, q * LANES)
            y_scr[:, cols] = xc * pair_wide(direct_ref[...], q)
            u_scr[:, cols] = (xc * pair_wide(step, q)).astype(bf16)
            state = None
            for k in range(blocks):
                rows = slice(k * L, (k + 1) * L)
                run = runs[k]
                end = run[L - 1 : L]
                leave = pair_wide(jnp.exp(end - run), q)
                added = lax.dot_general(
                    bb_scr[rows, ncol : ncol + LANES],
                    (u_scr[rows, cols].astype(f32) * leave).astype(bf16),
                    (((0,), (0,)), ((), ())), preferred_element_type=f32,
                )
                state = added if k == 0 else state * pair_wide(jnp.exp(end), q) + added
                if k < blocks - 1:
                    st_scr[k, :, cols] = state.astype(bf16)
            state = state.astype(bf16)
            for r in range(STATE_WIDTH // 16):
                pack[r * panels + q] = state[r * 16 : (r + 1) * 16]

    def send_state(d, carry):
        t = lax.rem(s + d, n_sp)
        remote(pack.at[t], xin.at[s], ex_s, ex_r, (t, x)).start()
        return carry

    lax.fori_loop(1, n_sp, send_state, 0)
    xin[s] = pack[s]

    for g in range(groups):
        col = g * STATE_WIDTH
        cc_scr[:, col : col + LANES] = conv(c_scr, tailc, fc_ref, col).astype(bf16)
    lane = lax.broadcasted_iota(jnp.int32, (L, LANES), 1)
    for g in range(groups):
        ncol = g * STATE_WIDTH
        for k in range(blocks):
            rows = slice(k * L, (k + 1) * L)
            cb = cc_scr[rows, ncol : ncol + LANES]
            bb = bb_scr[rows, ncol : ncol + LANES]
            prod = lax.dot_general(cb, bb, (((1,), (1,)), ((), ())), preferred_element_type=f32)
            run = runs[k]
            run_t = runs_t[k]
            enter = jnp.exp(run)
            for p in range(pairs):
                q = g * pairs + p
                cols = slice(q * LANES, (q + 1) * LANES)
                u = u_scr[rows, cols]
                mats = []
                for h in (2 * q, 2 * q + 1):
                    diff = jnp.where(causal, run[:, h : h + 1] - run_t[h : h + 1, :], -1e30)
                    mats.append((prod * jnp.exp(diff)).astype(bf16))
                zero = jnp.zeros_like(u)
                both = jnp.concatenate(
                    [jnp.where(lane < HEAD_DIM, u, zero), jnp.where(lane < HEAD_DIM, zero, u)], axis=0
                )
                out = jnp.dot(jnp.concatenate(mats, axis=1), both, preferred_element_type=f32)
                if k > 0:
                    out = out + pair_wide(enter, q) * jnp.dot(
                        cb, st_scr[k - 1, :, cols], preferred_element_type=f32
                    )
                y_scr[rows, cols] = y_scr[rows, cols] + out

    def got(ref, ss, rr):
        return remote(ref, ref, ss, rr, (lax.rem(s + 1, n_sp), x))

    got(logs_in.at[pl.ds(0, n_sp - 1)], log_s, log_r).wait_recv()
    got(xin.at[pl.ds(0, n_sp - 1)], ex_s, ex_r).wait_recv()
    factors = jnp.exp(logs_in[...].reshape(n_sp, LANES))
    logs_in[...] = factors.reshape(n_sp, 1, LANES)

    def turn(i, now):
        eout[i] = now.astype(bf16)
        return logs_in[i] * now + xin[i].astype(f32)

    lax.fori_loop(0, n_sp, turn, jnp.zeros((16, LANES), f32), unroll=8)

    def send_enter(d, carry):
        t = lax.rem(s + d, n_sp)
        remote(eout.at[t], ein.at[s], en_s, en_r, (t, x)).start()
        return carry

    lax.fori_loop(1, n_sp, send_enter, 0)
    ein[s] = eout[s]
    here[4].wait()
    here[5].wait()
    got(ein.at[pl.ds(0, n_sp - 1)], en_s, en_r).wait_recv()

    enters = [
        jnp.concatenate([ein[r * panels + q] for r in range(STATE_WIDTH // 16)], axis=0) for q in range(panels)
    ]

    def rs_copy(k):
        src, dst, target = (
            (part_scr.at[2, 0], relay.at[0], right), (part_scr.at[2, 1], relay.at[1], left),
            (part_scr.at[1, 0], rs_in.at[0, 0], right), (part_scr.at[1, 1], rs_in.at[0, 1], right),
            (part_scr.at[3, 0], rs_in.at[1, 0], left), (part_scr.at[3, 1], rs_in.at[1, 1], left),
        )[k]
        return remote(src, dst, rs_s.at[k], rs_r.at[k], (s, target))

    def mix_rows(i, carry):
        d = jnp.where(i == 0, 2, jnp.where(i == 1, 1, jnp.where(i == 2, 3, 0)))
        rows = pl.ds(pl.multiple_of(lax.rem(x + d, n_tp) * rows_here, 32), rows_here)
        enter = jnp.exp(run_scr[rows, :])
        normed = []
        for g in range(groups):
            cb = cc_scr[rows, g * STATE_WIDTH : (g + 1) * STATE_WIDTH]
            cols = slice(g * per, (g + 1) * per)
            read = jnp.concatenate(
                [
                    jnp.dot(cb, enters[g * pairs + p], preferred_element_type=f32) * pair_wide(enter, g * pairs + p)
                    for p in range(pairs)
                ],
                axis=1,
            )
            gated = (y_scr[rows, cols] + read) * gs_scr[rows, cols]
            scale = lax.rsqrt(jnp.mean(gated * gated, axis=-1, keepdims=True) + EPS)
            normed.append((gated * scale * gain_ref[:, cols]).astype(bf16))
        out = jnp.dot(jnp.concatenate(normed, axis=1), wout_scr[...], preferred_element_type=f32).astype(bf16)
        part_scr[d, 0] = out[:, :half]
        part_scr[d, 1] = out[:, half:]

        @pl.when(i == 0)
        def _():
            rs_copy(0).start()
            rs_copy(1).start()

        @pl.when(i == 1)
        def _():
            rs_copy(3).start()

        @pl.when(i == 2)
        def _():
            rs_copy(4).start()

        return carry

    lax.fori_loop(0, n_tp, mix_rows, 0)
    for k, d in ((0, 1), (1, 3)):
        rs_copy(k).wait_recv()
        part_scr[d, k] = (part_scr[d, k].astype(f32) + relay[k].astype(f32)).astype(bf16)
        rs_copy((2, 5)[k]).start()
    send_weight(2)
    mixed = [part_scr[0, h].astype(f32) for h in range(2)]
    for k in (3, 4, 2, 5):
        rs_copy(k).wait_recv()
        mixed[k % 2] = mixed[k % 2] + rs_in[(k - 2) // 2, k % 2].astype(f32)
    mixed = jnp.concatenate(mixed, axis=1)
    middle = norm_rows(ALPHA * res_scr[...].astype(f32) + mixed, g1_ref[...], b1_ref[...]).astype(bf16).astype(f32)
    for c in range(chunks):
        tmpf[pl.ds(c, rows_here, stride=chunks), :] = middle[:, c * LANES : (c + 1) * LANES]
    mid3[...] = tmpf[0 : rows_here * chunks, :].reshape(rows_here, chunks, LANES).astype(bf16)

    def fill(t):
        for k in range(CAP):
            out5[t, k] = mid3[src_ref[t * CAP + k]]

    stay = jnp.where(is_root, 0, 1)

    def send_plane(i, away):
        plane = lax.rem(z + SHIFTS[i], PLANES)
        for m in range(Y_CORES // 2):
            t = plane * Y_CORES + lax.rem(yc + 2 * m + (1 - stay if away else stay), Y_CORES)
            slot = (i * 2 + away) * Y_CORES + yc
            fill(t)

            def send():
                remote(
                    out5.at[t], rin.at[slot], d_s.at[PLANES if away else i], d_r.at[i // 2],
                    (t, beyond(plane) if away else x),
                ).start()

            if SHIFTS[i] == 0 and m == 0 and not away:

                @pl.when(is_root)
                def _():
                    rin[slot] = out5[s]

                pl.when(jnp.logical_not(is_root))(send)
            else:
                send()

    def sent_plane(i):
        def wait(count):
            got(out5.at[pl.ds(0, count)], d_s.at[i], d_r.at[0]).wait_send()

        if i < PLANES and SHIFTS[i] == 0:

            @pl.when(is_root)
            def _():
                wait(Y_CORES // 2 - 1)

            @pl.when(jnp.logical_not(is_root))
            def _():
                wait(Y_CORES // 2)

        else:
            wait(Y_CORES // 2 if i < PLANES else n_sp // 2)

    def next_weight(k):
        @pl.when(is_root)
        def _():
            sent_weight(k - 2, True)

        @pl.when(jnp.logical_not(is_root))
        def _():
            sent_weight(k - 2, False)

        send_weight(k)

    for i in range(PLANES):
        send_plane(i, 1)
    send_weight(3)
    send_weight(4)
    send_plane(0, 0)
    send_plane(1, 0)
    for i in range(2, PLANES):
        sent_plane(i - 2)
        send_plane(i, 0)
        if i == 5:
            next_weight(5)
    next_weight(6)
    quarter = 4 * Y_CORES
    n = quarter * CAP
    senders = 2 * n_sp
    own_plane = SHIFTS.index(0)
    own_chunk = own_plane // 2

    def landed(m, first, count, sem):
        ref = wbuf.at[m, pl.ds(0, n_tp - 1), pl.ds(first, count)]
        remote(ref, ref, w_s.at[0], w_r.at[sem], (lax.rem(s + 1, n_sp), x)).wait_recv()

    @pl.when(is_root)
    def _():
        own_weight(0).wait()
        landed(0, 0, model, 0)

        def expert_chunk(ci, carry):
            base = ci * quarter

            @pl.when(ci != own_chunk)
            def _():
                got(rin.at[pl.ds(0, quarter)], d_s.at[0], d_r.at[ci]).wait_recv()

            @pl.when(ci == own_chunk)
            def _():
                got(rin.at[pl.ds(0, quarter - 1)], d_s.at[0], d_r.at[ci]).wait_recv()

            tmpf[0 : n * chunks, :] = rin[pl.ds(base, quarter)].astype(f32).reshape(n * chunks, LANES)
            rows = pl.ds(pl.multiple_of(ci * n, n), n)
            for c in range(chunks):
                xrow[rows, c * LANES : (c + 1) * LANES] = tmpf[pl.ds(c, n, stride=chunks), :].astype(bf16)
            for t in range(n_tp):
                gated_scr[t, rows, :] = jnp.dot(xrow[rows, :], wbuf[0, t], preferred_element_type=f32)
            return carry

        lax.fori_loop(0, 4, expert_chunk, 0)
        own_weight(1).wait()
        landed(1, 0, model, 1)

        def expert_up(t, carry):
            up = jnp.dot(xrow[...], wbuf[1, t], preferred_element_type=f32)
            hid[t] = (silu(gated_scr[t]) * up).astype(bf16)
            return carry

        lax.fori_loop(0, n_tp, expert_up, 0)
        next_weight(7)
        next_weight(8)
        own_weight(2).wait()

        fourth = chunks // 4

        def answer_part(h, carry):
            landed(2, h * piece, piece, 2 + h)
            for o in range(fourth // 2):
                ans = None
                for t in range(n_tp):
                    part = lax.dot_general(
                        hid[t], wbuf[2, t, pl.ds(pl.multiple_of(h * piece + 2 * o * LANES, 2 * LANES), 2 * LANES), :],
                        (((1,), (1,)), ((), ())), preferred_element_type=f32,
                    )
                    ans = part if ans is None else ans + part
                tmpf[pl.ds(2 * o, senders * CAP, stride=fourth), :] = ans[:, :LANES]
                tmpf[pl.ds(2 * o + 1, senders * CAP, stride=fourth), :] = ans[:, LANES:]
            ansb[h] = tmpf[0 : senders * CAP * fourth, :].reshape(senders, CAP, fourth, LANES).astype(bf16)

            for i in range(PLANES):
                base = lax.rem(z + PLANES - SHIFTS[i], PLANES) * Y_CORES
                for g in range(2):
                    for j in range(1 if i == own_plane and g == 0 else 0, Y_CORES):
                        y = lax.rem(yc + j, Y_CORES)
                        slot = (i * 2 + g) * Y_CORES + y
                        remote(
                            ansb.at[h, slot], fin.at[h, s], f_s, f_r.at[h], (base + y, x if g == 0 else xp)
                        ).start()
            fin[h, s] = ansb[h, own_plane * 2 * Y_CORES + yc]
            return carry

        lax.fori_loop(0, 4, answer_part, 0)

    @pl.when(jnp.logical_not(is_root))
    def _():
        next_weight(7)
        next_weight(8)

    fourth = chunks // 4
    for h in range(4):

        @pl.when(is_root)
        def _():
            got(fin.at[h, pl.ds(0, n_sp - 1)], f_s, f_r.at[h]).wait_recv()

        @pl.when(jnp.logical_not(is_root))
        def _():
            got(fin.at[h], f_s, f_r.at[h]).wait_recv()

        def combine(r, carry):
            total = ALPHA * mid3[r, h * fourth : (h + 1) * fourth].astype(f32)
            ffn = None
            for k in range(2):
                slot = slot_ref[k * rows_here + r]
                one = stage[slot // CAP, lax.rem(slot, CAP)].astype(f32) * rw_ref[k, r]
                ffn = one if ffn is None else ffn + one
            tmpf[pl.ds(pl.multiple_of(r * chunks + h * fourth, fourth), fourth), :] = total + ffn
            return carry

        stage[...] = fin[h]
        lax.fori_loop(0, rows_here, combine, 0, unroll=8)
    total = jnp.concatenate([tmpf[pl.ds(c, rows_here, stride=chunks), :] for c in range(chunks)], axis=1)
    o_ref[...] = norm_rows(total, g2_ref[...], b2_ref[...]).astype(bf16)

    @pl.when(s < n_sp - 1)
    def _():
        for a, t, i in tails:
            tail_copy(a, t, i, s + 1).wait_send()

    got(logs_in.at[pl.ds(0, n_sp - 1)], log_s, log_r).wait_send()
    got(xin.at[pl.ds(0, n_sp - 1)], ex_s, ex_r).wait_send()
    got(ein.at[pl.ds(0, n_sp - 1)], en_s, en_r).wait_send()
    for k in range(6):
        rs_copy(k).wait_send()
    for i in range(PLANES - 2, PLANES + 1):
        sent_plane(i)

    @pl.when(is_root)
    def _():
        for k in (0, 1, 2, 7, 8):
            sent_weight(k, True)
        got(ansb.at[pl.ds(0, 4), pl.ds(0, senders - 1)], f_s, f_r.at[0]).wait_send()

    @pl.when(jnp.logical_not(is_root))
    def _():
        for k in (0, 1, 2, 7, 8):
            sent_weight(k, False)


def slot_layout(by_rank):
    top, rows = by_rank.shape
    flat = by_rank.reshape(-1)
    row = jnp.arange(top * rows, dtype=jnp.int32) % rows
    earlier = row[:, None] > row[None, :]
    rank = jnp.sum((earlier & (flat[:, None] == flat[None, :])).astype(jnp.int32), axis=1)
    slots = flat * CAP + rank
    hit = slots[:, None] == jnp.arange(N_EXPERTS * CAP, dtype=jnp.int32)[None, :]
    source = jnp.sum(jnp.where(hit, row[:, None], 0), axis=0)
    return slots, source


def shards(
    head_input_values, group_input_vectors, group_readout_vectors, output_gate_values,
    step_size_logits, extra_log_decay, head_input_filter, input_vector_filter,
    readout_vector_filter, step_size_bias, head_rate_logarithm, direct_path_weight,
    group_norm_scale, mixer_output_weight, residual, first_norm_scale, first_norm_bias,
    routes, routing_weight, expert_gate_weight, expert_up_weight, expert_down_weight,
    final_norm_scale, final_norm_bias,
):
    n_sp, n_tp = lax.axis_size("sp"), lax.axis_size("tp")
    length, width = head_input_values.shape
    gw = group_input_vectors.shape[1]
    heads = step_size_logits.shape[1]
    rows_here, model = residual.shape
    hidden = expert_gate_weight.shape[2]
    chunks = model // LANES
    panels = width // LANES
    slots, source = slot_layout(routes.T)
    dma = pltpu.SemaphoreType.DMA
    root_rows = 2 * n_sp * CAP
    return pl.pallas_call(
        layer_kernel,
        out_shape=jax.ShapeDtypeStruct((rows_here, model), bf16),
        in_specs=[HBM] * 4 + [VMEM] * 9 + [HBM] * 2 + [VMEM] * 2 + [SMEM] * 3 + [HBM] * 3 + [VMEM] * 2,
        out_specs=VMEM,
        scratch_shapes=[
            pltpu.VMEM((length, width), bf16),
            pltpu.VMEM((length, gw), bf16),
            pltpu.VMEM((length, gw), bf16),
            pltpu.VMEM((length, width), bf16),
            pltpu.VMEM((width, model), bf16),
            pltpu.VMEM((rows_here, model), bf16),
            pltpu.VMEM((8, width), bf16),
            pltpu.VMEM((8, gw), bf16),
            pltpu.VMEM((8, gw), bf16),
            pltpu.VMEM((length + 8, LANES), f32),
            pltpu.VMEM((length, width), f32),
            pltpu.VMEM((length, width), bf16),
            pltpu.VMEM((length, gw), bf16),
            pltpu.VMEM((length, gw), bf16),
            pltpu.VMEM((length, heads), f32),
            pltpu.VMEM((2, STATE_WIDTH, width), bf16),
            pltpu.VMEM((length, width), f32),
            pltpu.VMEM((panels, 1, LANES), f32),
            pltpu.VMEM((n_sp, 1, LANES), f32),
            pltpu.VMEM((n_sp, 16, LANES), bf16),
            pltpu.VMEM((n_sp, 16, LANES), bf16),
            pltpu.VMEM((n_sp, 16, LANES), bf16),
            pltpu.VMEM((n_sp, 16, LANES), bf16),
            pltpu.VMEM((n_tp, 2, rows_here, model // 2), bf16),
            pltpu.VMEM((2, rows_here, model // 2), bf16),
            pltpu.VMEM((2, 2, rows_here, model // 2), bf16),
            pltpu.VMEM((rows_here, chunks, LANES), bf16),
            pltpu.VMEM((root_rows * chunks // 2, LANES), f32),
            pltpu.VMEM((n_sp, CAP, chunks, LANES), bf16),
            pltpu.VMEM((2 * n_sp, CAP, chunks, LANES), bf16),
            pltpu.VMEM((root_rows, model), bf16),
            pltpu.VMEM((n_tp, root_rows, hidden), f32),
            pltpu.VMEM((n_tp, root_rows, hidden), bf16),
            pltpu.VMEM((4, 2 * n_sp, CAP, chunks // 4, LANES), bf16),
            pltpu.VMEM((4, n_sp, CAP, chunks // 4, LANES), bf16),
            pltpu.VMEM((n_sp, CAP, chunks // 4, LANES), bf16),
            pltpu.VMEM((3, n_tp, model, hidden), bf16),
            dma((6,)), dma((3,)), dma((3,)), dma((3,)), dma, dma, dma, dma, dma, dma,
            dma((6,)), dma((6,)), dma((9,)), dma((6,)), dma((PLANES + 1,)), dma((4,)), dma, dma((4,)),
        ],
        compiler_params=pltpu.CompilerParams(
            collective_id=0, has_side_effects=True, vmem_limit_bytes=60 * 1024 * 1024
        ),
        name="layer",
    )(
        head_input_values, group_input_vectors, group_readout_vectors, output_gate_values,
        step_size_logits.T, extra_log_decay.T, head_input_filter, input_vector_filter, readout_vector_filter,
        step_size_bias.reshape(1, heads), head_rate_logarithm.reshape(1, heads), direct_path_weight.reshape(1, heads),
        group_norm_scale.astype(f32).reshape(1, width), mixer_output_weight, residual,
        first_norm_scale.reshape(1, model), first_norm_bias.reshape(1, model),
        source, slots, routing_weight.T,
        expert_gate_weight, expert_up_weight, expert_down_weight,
        final_norm_scale.reshape(1, model), final_norm_bias.reshape(1, model),
    )


def solution(mesh):
    in_specs = (
        P("sp", "tp"), P("sp", "tp"), P("sp", "tp"), P("sp", "tp"), P("sp", "tp"), P("sp", "tp"),
        P(None, "tp"), P(None, "tp"), P(None, "tp"), P("tp"), P("tp"), P("tp"), P("tp"),
        P("tp", None), P(("sp", "tp"), None), P(), P(), P(("sp", "tp"), None), P(("sp", "tp"), None),
        P("sp", None, "tp"), P("sp", None, "tp"), P("sp", None, "tp"), P(), P(),
    )
    out_specs = P(("sp", "tp"), None)
    return jax.shard_map(shards, mesh=mesh, in_specs=in_specs, out_specs=out_specs, check_vma=False)
```

```python
import functools

import jax
import jax.numpy as jnp
from jax import lax
from jax.experimental import pallas as pl
from jax.experimental.pallas import tpu as pltpu
from jax.sharding import PartitionSpec as P

HEAD_DIM = 64
STATE_WIDTH = 128
BLOCK_LENGTH = 128
EPS = 1e-05
ALPHA = 8.0**0.25
LANES = 128
CAP = 5
Y_CORES = 8
PLANES = 8

f32 = jnp.float32
bf16 = jnp.bfloat16
MESH = pl.DeviceIdType.MESH
VMEM = pl.BlockSpec(memory_space=pltpu.VMEM)
SMEM = pl.BlockSpec(memory_space=pltpu.SMEM)
HBM = pl.BlockSpec(memory_space=pltpu.MemorySpace.HBM)


def silu(v):
    return v * (1.0 / (1.0 + jnp.exp(-v)))


def pair_wide(values, pair):
    rows = values.shape[0]
    lane = lax.broadcasted_iota(jnp.int32, (rows, LANES), 1)
    a = jnp.broadcast_to(values[:, 2 * pair : 2 * pair + 1], (rows, LANES))
    b = jnp.broadcast_to(values[:, 2 * pair + 1 : 2 * pair + 2], (rows, LANES))
    return jnp.where(lane < HEAD_DIM, a, b)


def norm_rows(values, gain, bias):
    centred = values - jnp.mean(values, axis=-1, keepdims=True)
    spread = jnp.mean(centred * centred, axis=-1, keepdims=True)
    return centred * lax.rsqrt(spread + EPS) * gain + bias


SHIFTS = (3, 5, 4, 0, 2, 6, 1, 7)


def layer_kernel(
    x_hbm, b_hbm, c_hbm, gate_hbm, logit_ref, extra_ref, fx_ref, fb_ref, fc_ref,
    bias_ref, rate_ref, direct_ref, gain_ref, wout_hbm, res_hbm, g1_ref, b1_ref,
    route_ref, rw_ref, wg_hbm, wu_hbm, wd_hbm, g2_ref, b2_ref,
    o_ref,
    x_scr, b_scr, c_scr, gate_scr, wout_scr, res_scr,
    tailx, tailb, tailc, pad_scr, y_scr, u_scr, bb_scr, cc_scr, run_scr, st_scr, gs_scr,
    logs_out, logs_in, pack, xin, eout, ein,
    part_scr, relay, rs_in, mid3, tmpf, out5, rin, xrow, gated_scr, hid, ansb, fin, stage, wbuf, table, src_ref, slot_ref,
    lsem, wlsem, tail_s, tail_r, log_s, log_r, ex_s, ex_r, en_s, en_r, rs_s, rs_r, w_s, w_r, d_s, d_r, f_s, f_r,
):
    n_sp, n_tp = 64, 4
    s = lax.axis_index("sp")
    x = lax.axis_index("tp")
    z = s // Y_CORES
    yc = lax.rem(s, Y_CORES)
    core = lax.rem(s, 2)
    odd = lax.rem(x, 2)
    right, left = lax.rem(x + 1, n_tp), lax.rem(x + n_tp - 1, n_tp)

    def beyond(plane):
        return jnp.where(lax.rem(plane, 2) == 0, right, left)

    xp = jnp.where(lax.rem(z, 2) == 0, left, right)
    is_root = core == odd
    length, width = x_scr.shape
    gw = b_scr.shape[1]
    taps = fx_ref.shape[0]
    heads = logit_ref.shape[0]
    groups = gw // STATE_WIDTH
    per = width // groups
    pairs = per // LANES
    panels = width // LANES
    L = BLOCK_LENGTH
    blocks = length // L
    rows_here, model = o_ref.shape
    chunks = model // LANES

    def remote(src, dst, ss, rr, dev):
        return pltpu.make_async_remote_copy(
            src_ref=src, dst_ref=dst, send_sem=ss, recv_sem=rr, device_id=dev, device_id_type=MESH
        )

    here = [
        pltpu.make_async_copy(a, b, lsem.at[i])
        for i, (a, b) in enumerate(
            ((x_hbm, x_scr), (b_hbm, b_scr), (c_hbm, c_scr), (gate_hbm, gate_scr), (wout_hbm, wout_scr), (res_hbm, res_scr))
        )
    ]
    for copy in here:
        copy.start()
    experts_w = (wg_hbm, wu_hbm, wd_hbm)
    half = model // 2

    def own_weight(m):
        return pltpu.make_async_copy(experts_w[m].at[0], wbuf.at[m, x], wlsem.at[m])

    @pl.when(is_root)
    def _():
        for m in range(3):
            own_weight(m).start()

    piece = model // 4
    pieces = [(0, 0, model, 0)] + [(1, q * piece, piece, 1) for q in range(4)] + [
        (2, q * piece, piece, 2 + q) for q in range(4)
    ]

    def send_weight(k):
        m, first, count, sem = pieces[k]
        rows = pl.ds(first, count)

        def send(target):
            remote(experts_w[m].at[0, rows], wbuf.at[m, x, rows], w_s.at[k], w_r.at[sem], (s, target)).start()

        @pl.when(is_root)
        def _():
            send(lax.rem(x + 2, n_tp))

        @pl.when(jnp.logical_not(is_root))
        def _():
            send(lax.rem(x + 1, n_tp))
            send(lax.rem(x + 3, n_tp))

    def sent_weight(k, root):
        m, first, count, sem = pieces[k]
        ref = wbuf.at[m, 0, pl.ds(first, count)] if root else wbuf.at[m, pl.ds(0, 2), pl.ds(first, count)]
        remote(ref, ref, w_s.at[k], w_r.at[sem], (lax.rem(s + 1, n_sp), x)).wait_send()

    barrier = pltpu.get_barrier_semaphore()

    def greet(d, carry):
        t = lax.rem(s + d, n_sp)
        pl.semaphore_signal(barrier, inc=1, device_id=(t, x), device_id_type=MESH)
        return carry

    lax.fori_loop(1, n_sp, greet, 0)

    def greet_experts(k, carry):
        t = 2 * k + 1 - odd
        pl.semaphore_signal(barrier, inc=1, device_id=(t, beyond(t // Y_CORES)), device_id_type=MESH)
        return carry

    lax.fori_loop(0, n_sp // 2, greet_experts, 0)

    @pl.when(is_root)
    def _():
        def greet_senders(t, carry):
            pl.semaphore_signal(barrier, inc=1, device_id=(t, xp), device_id_type=MESH)
            return carry

        lax.fori_loop(0, n_sp, greet_senders, 0)

    for d in range(1, n_tp):
        pl.semaphore_signal(barrier, inc=1, device_id=(s, lax.rem(x + d, n_tp)), device_id_type=MESH)

    v = logit_ref[...] + bias_ref[...].T
    step_t = jnp.maximum(v, 0.0) + jnp.log(1.0 + jnp.exp(-jnp.abs(v)))
    decay_t = -step_t * jnp.exp(rate_ref[...].T) + extra_ref[...]
    step = step_t.T
    ti = lax.broadcasted_iota(jnp.int32, (L, L), 0)
    si = lax.broadcasted_iota(jnp.int32, (L, L), 1)
    causal = ti >= si
    tri = (ti <= si).astype(f32)
    runs, runs_t = [], []
    before = jnp.zeros((1, heads), f32)
    for k in range(blocks):
        r_t = jnp.dot(decay_t[:, k * L : (k + 1) * L], tri, precision=lax.Precision.HIGHEST, preferred_element_type=f32)
        r = r_t.T
        runs_t.append(r_t)
        runs.append(r)
        run_scr[k * L : (k + 1) * L, :] = r + before
        before = before + r[L - 1 : L]
    for p in range(panels):
        logs_out[p] = pair_wide(before, p)
    experts = n_sp
    name = lax.broadcasted_iota(jnp.int32, (experts, rows_here), 0)
    named = [(name == route_ref[k : k + 1, :]).astype(f32) for k in range(2)]
    both = named[0] + named[1]
    ri = lax.broadcasted_iota(jnp.int32, (rows_here, rows_here), 0)
    rj = lax.broadcasted_iota(jnp.int32, (rows_here, rows_here), 1)
    earlier = jnp.dot(both.astype(bf16), (ri < rj).astype(bf16), preferred_element_type=f32)
    for k in range(2):
        rank = jnp.sum(named[k] * earlier, axis=0, keepdims=True)
        table[1, k : k + 1, 0:rows_here] = route_ref[k : k + 1, :] * CAP + rank.astype(jnp.int32)
    both_t, earlier_t = both.T, earlier.T
    token = lax.broadcasted_iota(jnp.int32, (rows_here, experts), 0).astype(f32)
    for k in range(CAP):
        here_k = jnp.logical_and(both_t > 0.5, jnp.abs(earlier_t - k) < 0.5)
        table[0, k : k + 1, 0:experts] = jnp.sum(jnp.where(here_k, token, 0.0), axis=0, keepdims=True).astype(jnp.int32)
    tables = [
        pltpu.make_async_copy(table.at[0], src_ref, lsem.at[6]),
        pltpu.make_async_copy(table.at[1], slot_ref, lsem.at[7]),
    ]
    here[3].wait()

    def gate_rows(i, carry):
        rows = pl.ds(pl.multiple_of(i * 32, 32), 32)
        gs_scr[rows, :] = silu(gate_scr[rows, :].astype(f32))
        return carry

    lax.fori_loop(0, length // 32, gate_rows, 0)
    for copy in here[:3]:
        copy.wait()
    for copy in tables:
        copy.start()

    pl.semaphore_wait(barrier, n_sp - 1 + n_tp - 1 + n_sp // 2 + jnp.where(is_root, n_sp, 0))

    tails = (
        (x_scr, tailx, 0), (b_scr, tailb, 1), (c_scr, tailc, 2),
    )

    def tail_copy(a, t, i, target):
        return remote(a.at[pl.ds(length - 8, 8)], t, tail_s.at[i], tail_r.at[i], (target, x))

    @pl.when(s < n_sp - 1)
    def _():
        for a, t, i in tails:
            tail_copy(a, t, i, s + 1).start()

    def send_log(d, carry):
        t = lax.rem(s + d, n_sp)
        remote(logs_out.at[lax.rem(t, panels)], logs_in.at[s], log_s, log_r, (t, x)).start()
        return carry

    lax.fori_loop(1, n_sp, send_log, 0)
    logs_in[s] = logs_out[lax.rem(s, panels)]

    send_weight(0)
    send_weight(1)

    @pl.when(s == 0)
    def _():
        for _, t, _i in tails:
            t[...] = jnp.zeros_like(t)

    @pl.when(s > 0)
    def _():
        for a, t, i in tails:
            tail_copy(a, t, i, s - 1).wait_recv()

    def conv(raw_ref, tail_ref, filt_ref, col):
        pad_scr[0:8, :] = tail_ref[:, col : col + LANES].astype(f32)
        pad_scr[8 : 8 + length, :] = raw_ref[:, col : col + LANES].astype(f32)
        acc = None
        for o in range(taps):
            start = 8 - (taps - 1) + o
            part = pad_scr[start : start + length, :] * filt_ref[o : o + 1, col : col + LANES].astype(f32)
            acc = part if acc is None else acc + part
        return silu(acc)

    for g in range(groups):
        col = g * STATE_WIDTH
        bb_scr[:, col : col + LANES] = conv(b_scr, tailb, fb_ref, col).astype(bf16)
    for g in range(groups):
        ncol = g * STATE_WIDTH
        for p in range(pairs):
            q = g * pairs + p
            cols = slice(q * LANES, (q + 1) * LANES)
            xc = conv(x_scr, tailx, fx_ref, q * LANES)
            y_scr[:, cols] = xc * pair_wide(direct_ref[...], q)
            u_scr[:, cols] = (xc * pair_wide(step, q)).astype(bf16)
            state = None
            for k in range(blocks):
                rows = slice(k * L, (k + 1) * L)
                run = runs[k]
                end = run[L - 1 : L]
                leave = pair_wide(jnp.exp(end - run), q)
                added = lax.dot_general(
                    bb_scr[rows, ncol : ncol + LANES],
                    (u_scr[rows, cols].astype(f32) * leave).astype(bf16),
                    (((0,), (0,)), ((), ())), preferred_element_type=f32,
                )
                state = added if k == 0 else state * pair_wide(jnp.exp(end), q) + added
                if k < blocks - 1:
                    st_scr[k, :, cols] = state.astype(bf16)
            state = state.astype(bf16)
            for r in range(STATE_WIDTH // 16):
                pack[r * panels + q] = state[r * 16 : (r + 1) * 16]

    def send_state(d, carry):
        t = lax.rem(s + d, n_sp)
        remote(pack.at[t], xin.at[s], ex_s, ex_r, (t, x)).start()
        return carry

    lax.fori_loop(1, n_sp, send_state, 0)
    xin[s] = pack[s]

    for g in range(groups):
        col = g * STATE_WIDTH
        cc_scr[:, col : col + LANES] = conv(c_scr, tailc, fc_ref, col).astype(bf16)
    lane = lax.broadcasted_iota(jnp.int32, (L, LANES), 1)
    for g in range(groups):
        ncol = g * STATE_WIDTH
        for k in range(blocks):
            rows = slice(k * L, (k + 1) * L)
            cb = cc_scr[rows, ncol : ncol + LANES]
            bb = bb_scr[rows, ncol : ncol + LANES]
            prod = lax.dot_general(cb, bb, (((1,), (1,)), ((), ())), preferred_element_type=f32)
            run = runs[k]
            run_t = runs_t[k]
            enter = jnp.exp(run)
            for p in range(pairs):
                q = g * pairs + p
                cols = slice(q * LANES, (q + 1) * LANES)
                u = u_scr[rows, cols]
                mats = []
                for h in (2 * q, 2 * q + 1):
                    diff = jnp.where(causal, run[:, h : h + 1] - run_t[h : h + 1, :], -1e30)
                    mats.append((prod * jnp.exp(diff)).astype(bf16))
                zero = jnp.zeros_like(u)
                both = jnp.concatenate(
                    [jnp.where(lane < HEAD_DIM, u, zero), jnp.where(lane < HEAD_DIM, zero, u)], axis=0
                )
                out = jnp.dot(jnp.concatenate(mats, axis=1), both, preferred_element_type=f32)
                if k > 0:
                    out = out + pair_wide(enter, q) * jnp.dot(
                        cb, st_scr[k - 1, :, cols], preferred_element_type=f32
                    )
                y_scr[rows, cols] = y_scr[rows, cols] + out

    def got(ref, ss, rr):
        return remote(ref, ref, ss, rr, (lax.rem(s + 1, n_sp), x))

    got(logs_in.at[pl.ds(0, n_sp - 1)], log_s, log_r).wait_recv()
    got(xin.at[pl.ds(0, n_sp - 1)], ex_s, ex_r).wait_recv()
    factors = jnp.exp(logs_in[...].reshape(n_sp, LANES))
    logs_in[...] = factors.reshape(n_sp, 1, LANES)

    def turn(i, now):
        eout[i] = now.astype(bf16)
        return logs_in[i] * now + xin[i].astype(f32)

    lax.fori_loop(0, n_sp, turn, jnp.zeros((16, LANES), f32), unroll=8)

    def send_enter(d, carry):
        t = lax.rem(s + d, n_sp)
        remote(eout.at[t], ein.at[s], en_s, en_r, (t, x)).start()
        return carry

    lax.fori_loop(1, n_sp, send_enter, 0)
    ein[s] = eout[s]
    here[4].wait()
    here[5].wait()
    got(ein.at[pl.ds(0, n_sp - 1)], en_s, en_r).wait_recv()

    enters = [
        jnp.concatenate([ein[r * panels + q] for r in range(STATE_WIDTH // 16)], axis=0) for q in range(panels)
    ]

    def rs_copy(k):
        src, dst, target = (
            (part_scr.at[2, 0], relay.at[0], right), (part_scr.at[2, 1], relay.at[1], left),
            (part_scr.at[1, 0], rs_in.at[0, 0], right), (part_scr.at[1, 1], rs_in.at[0, 1], right),
            (part_scr.at[3, 0], rs_in.at[1, 0], left), (part_scr.at[3, 1], rs_in.at[1, 1], left),
        )[k]
        return remote(src, dst, rs_s.at[k], rs_r.at[k], (s, target))

    def mix_rows(i, carry):
        d = jnp.where(i == 0, 2, jnp.where(i == 1, 1, jnp.where(i == 2, 3, 0)))
        rows = pl.ds(pl.multiple_of(lax.rem(x + d, n_tp) * rows_here, 32), rows_here)
        enter = jnp.exp(run_scr[rows, :])
        normed = []
        for g in range(groups):
            cb = cc_scr[rows, g * STATE_WIDTH : (g + 1) * STATE_WIDTH]
            cols = slice(g * per, (g + 1) * per)
            read = jnp.concatenate(
                [
                    jnp.dot(cb, enters[g * pairs + p], preferred_element_type=f32) * pair_wide(enter, g * pairs + p)
                    for p in range(pairs)
                ],
                axis=1,
            )
            gated = (y_scr[rows, cols] + read) * gs_scr[rows, cols]
            scale = lax.rsqrt(jnp.mean(gated * gated, axis=-1, keepdims=True) + EPS)
            normed.append((gated * scale * gain_ref[:, cols]).astype(bf16))
        out = jnp.dot(jnp.concatenate(normed, axis=1), wout_scr[...], preferred_element_type=f32).astype(bf16)
        part_scr[d, 0] = out[:, :half]
        part_scr[d, 1] = out[:, half:]

        @pl.when(i == 0)
        def _():
            rs_copy(0).start()
            rs_copy(1).start()

        @pl.when(i == 1)
        def _():
            rs_copy(3).start()

        @pl.when(i == 2)
        def _():
            rs_copy(4).start()

        return carry

    lax.fori_loop(0, n_tp, mix_rows, 0)
    for k, d in ((0, 1), (1, 3)):
        rs_copy(k).wait_recv()
        part_scr[d, k] = (part_scr[d, k].astype(f32) + relay[k].astype(f32)).astype(bf16)
        rs_copy((2, 5)[k]).start()
    send_weight(2)
    mixed = [part_scr[0, h].astype(f32) for h in range(2)]
    for k in (3, 4, 2, 5):
        rs_copy(k).wait_recv()
        mixed[k % 2] = mixed[k % 2] + rs_in[(k - 2) // 2, k % 2].astype(f32)
    mixed = jnp.concatenate(mixed, axis=1)
    middle = norm_rows(ALPHA * res_scr[...].astype(f32) + mixed, g1_ref[...], b1_ref[...]).astype(bf16).astype(f32)
    for c in range(chunks):
        tmpf[pl.ds(c, rows_here, stride=chunks), :] = middle[:, c * LANES : (c + 1) * LANES]
    mid3[...] = tmpf[0 : rows_here * chunks, :].reshape(rows_here, chunks, LANES).astype(bf16)

    for copy in tables:
        copy.wait()
    def fill(t):
        for k in range(CAP):
            out5[t, k] = mid3[jnp.clip(src_ref[k, t], 0, rows_here - 1)]

    stay = jnp.where(is_root, 0, 1)

    def send_plane(i, away):
        plane = lax.rem(z + SHIFTS[i], PLANES)
        for m in range(Y_CORES // 2):
            t = plane * Y_CORES + lax.rem(yc + 2 * m + (1 - stay if away else stay), Y_CORES)
            slot = (i * 2 + away) * Y_CORES + yc
            fill(t)

            def send():
                remote(
                    out5.at[t], rin.at[slot], d_s.at[PLANES if away else i], d_r.at[i // 2],
                    (t, beyond(plane) if away else x),
                ).start()

            if SHIFTS[i] == 0 and m == 0 and not away:

                @pl.when(is_root)
                def _():
                    rin[slot] = out5[s]

                pl.when(jnp.logical_not(is_root))(send)
            else:
                send()

    def sent_plane(i):
        def wait(count):
            got(out5.at[pl.ds(0, count)], d_s.at[i], d_r.at[0]).wait_send()

        if i < PLANES and SHIFTS[i] == 0:

            @pl.when(is_root)
            def _():
                wait(Y_CORES // 2 - 1)

            @pl.when(jnp.logical_not(is_root))
            def _():
                wait(Y_CORES // 2)

        else:
            wait(Y_CORES // 2 if i < PLANES else n_sp // 2)

    def next_weight(k):
        @pl.when(is_root)
        def _():
            sent_weight(k - 2, True)

        @pl.when(jnp.logical_not(is_root))
        def _():
            sent_weight(k - 2, False)

        send_weight(k)

    for i in range(PLANES):
        send_plane(i, 1)
    send_weight(3)
    send_weight(4)
    send_plane(0, 0)
    send_plane(1, 0)
    for i in range(2, PLANES):
        sent_plane(i - 2)
        send_plane(i, 0)
        if i == 5:
            next_weight(5)
    next_weight(6)
    quarter = 4 * Y_CORES
    n = quarter * CAP
    senders = 2 * n_sp
    own_plane = SHIFTS.index(0)
    own_chunk = own_plane // 2

    def landed(m, first, count, sem):
        ref = wbuf.at[m, pl.ds(0, n_tp - 1), pl.ds(first, count)]
        remote(ref, ref, w_s.at[0], w_r.at[sem], (lax.rem(s + 1, n_sp), x)).wait_recv()

    @pl.when(is_root)
    def _():
        own_weight(0).wait()
        landed(0, 0, model, 0)

        def expert_chunk(ci, carry):
            base = ci * quarter

            @pl.when(ci != own_chunk)
            def _():
                got(rin.at[pl.ds(0, quarter)], d_s.at[0], d_r.at[ci]).wait_recv()

            @pl.when(ci == own_chunk)
            def _():
                got(rin.at[pl.ds(0, quarter - 1)], d_s.at[0], d_r.at[ci]).wait_recv()

            tmpf[0 : n * chunks, :] = rin[pl.ds(base, quarter)].astype(f32).reshape(n * chunks, LANES)
            rows = pl.ds(pl.multiple_of(ci * n, n), n)
            for c in range(chunks):
                xrow[rows, c * LANES : (c + 1) * LANES] = tmpf[pl.ds(c, n, stride=chunks), :].astype(bf16)
            for t in range(n_tp):
                gated_scr[t, rows, :] = jnp.dot(xrow[rows, :], wbuf[0, t], preferred_element_type=f32)
            return carry

        lax.fori_loop(0, 4, expert_chunk, 0)
        next_weight(7)
        own_weight(1).wait()
        landed(1, 0, model, 1)

        def expert_up(t, carry):
            up = jnp.dot(xrow[...], wbuf[1, t], preferred_element_type=f32)
            hid[t] = (silu(gated_scr[t]) * up).astype(bf16)
            return carry

        lax.fori_loop(0, n_tp, expert_up, 0)
        own_weight(2).wait()

        fourth = chunks // 4

        def answer_part(h, carry):
            landed(2, h * piece, piece, 2 + h)
            for o in range(fourth // 2):
                ans = None
                for t in range(n_tp):
                    part = lax.dot_general(
                        hid[t], wbuf[2, t, pl.ds(pl.multiple_of(h * piece + 2 * o * LANES, 2 * LANES), 2 * LANES), :],
                        (((1,), (1,)), ((), ())), preferred_element_type=f32,
                    )
                    ans = part if ans is None else ans + part
                tmpf[pl.ds(2 * o, senders * CAP, stride=fourth), :] = ans[:, :LANES]
                tmpf[pl.ds(2 * o + 1, senders * CAP, stride=fourth), :] = ans[:, LANES:]
            ansb[h] = tmpf[0 : senders * CAP * fourth, :].reshape(senders, CAP, fourth, LANES).astype(bf16)

            for i in range(PLANES):
                base = lax.rem(z + PLANES - SHIFTS[i], PLANES) * Y_CORES
                for g in range(2):
                    for j in range(1 if i == own_plane and g == 0 else 0, Y_CORES):
                        y = lax.rem(yc + j, Y_CORES)
                        slot = (i * 2 + g) * Y_CORES + y
                        remote(
                            ansb.at[h, slot], fin.at[h, s], f_s, f_r.at[h], (base + y, x if g == 0 else xp)
                        ).start()
            fin[h, s] = ansb[h, own_plane * 2 * Y_CORES + yc]

            @pl.when(h == 0)
            def _():
                next_weight(8)

            return carry

        lax.fori_loop(0, 4, answer_part, 0)

    @pl.when(jnp.logical_not(is_root))
    def _():
        next_weight(7)
        next_weight(8)

    fourth = chunks // 4
    for h in range(4):

        @pl.when(is_root)
        def _():
            got(fin.at[h, pl.ds(0, n_sp - 1)], f_s, f_r.at[h]).wait_recv()

        @pl.when(jnp.logical_not(is_root))
        def _():
            got(fin.at[h], f_s, f_r.at[h]).wait_recv()

        def combine(r, carry):
            total = ALPHA * mid3[r, h * fourth : (h + 1) * fourth].astype(f32)
            ffn = None
            for k in range(2):
                slot = jnp.clip(slot_ref[k, r], 0, n_sp * CAP - 1)
                one = stage[slot // CAP, lax.rem(slot, CAP)].astype(f32) * rw_ref[k, r]
                ffn = one if ffn is None else ffn + one
            tmpf[pl.ds(pl.multiple_of(r * chunks + h * fourth, fourth), fourth), :] = total + ffn
            return carry

        stage[...] = fin[h]
        lax.fori_loop(0, rows_here, combine, 0, unroll=8)
    total = jnp.concatenate([tmpf[pl.ds(c, rows_here, stride=chunks), :] for c in range(chunks)], axis=1)
    o_ref[...] = norm_rows(total, g2_ref[...], b2_ref[...]).astype(bf16)

    @pl.when(s < n_sp - 1)
    def _():
        for a, t, i in tails:
            tail_copy(a, t, i, s + 1).wait_send()

    got(logs_in.at[pl.ds(0, n_sp - 1)], log_s, log_r).wait_send()
    got(xin.at[pl.ds(0, n_sp - 1)], ex_s, ex_r).wait_send()
    got(ein.at[pl.ds(0, n_sp - 1)], en_s, en_r).wait_send()
    for k in range(6):
        rs_copy(k).wait_send()
    for i in range(PLANES - 2, PLANES + 1):
        sent_plane(i)

    @pl.when(is_root)
    def _():
        for k in (0, 1, 2, 7, 8):
            sent_weight(k, True)
        got(ansb.at[pl.ds(0, 4), pl.ds(0, senders - 1)], f_s, f_r.at[0]).wait_send()

    @pl.when(jnp.logical_not(is_root))
    def _():
        for k in (0, 1, 2, 7, 8):
            sent_weight(k, False)


def shards(
    head_input_values, group_input_vectors, group_readout_vectors, output_gate_values,
    step_size_logits, extra_log_decay, head_input_filter, input_vector_filter,
    readout_vector_filter, step_size_bias, head_rate_logarithm, direct_path_weight,
    group_norm_scale, mixer_output_weight, residual, first_norm_scale, first_norm_bias,
    routes, routing_weight, expert_gate_weight, expert_up_weight, expert_down_weight,
    final_norm_scale, final_norm_bias,
):
    n_sp, n_tp = lax.axis_size("sp"), lax.axis_size("tp")
    length, width = head_input_values.shape
    gw = group_input_vectors.shape[1]
    heads = step_size_logits.shape[1]
    rows_here, model = residual.shape
    hidden = expert_gate_weight.shape[2]
    chunks = model // LANES
    panels = width // LANES
    dma = pltpu.SemaphoreType.DMA
    root_rows = 2 * n_sp * CAP
    return pl.pallas_call(
        layer_kernel,
        out_shape=jax.ShapeDtypeStruct((rows_here, model), bf16),
        in_specs=[HBM] * 4 + [VMEM] * 9 + [HBM] * 2 + [VMEM] * 3 + [SMEM] + [HBM] * 3 + [VMEM] * 2,
        out_specs=VMEM,
        scratch_shapes=[
            pltpu.VMEM((length, width), bf16),
            pltpu.VMEM((length, gw), bf16),
            pltpu.VMEM((length, gw), bf16),
            pltpu.VMEM((length, width), bf16),
            pltpu.VMEM((width, model), bf16),
            pltpu.VMEM((rows_here, model), bf16),
            pltpu.VMEM((8, width), bf16),
            pltpu.VMEM((8, gw), bf16),
            pltpu.VMEM((8, gw), bf16),
            pltpu.VMEM((length + 8, LANES), f32),
            pltpu.VMEM((length, width), f32),
            pltpu.VMEM((length, width), bf16),
            pltpu.VMEM((length, gw), bf16),
            pltpu.VMEM((length, gw), bf16),
            pltpu.VMEM((length, heads), f32),
            pltpu.VMEM((2, STATE_WIDTH, width), bf16),
            pltpu.VMEM((length, width), f32),
            pltpu.VMEM((panels, 1, LANES), f32),
            pltpu.VMEM((n_sp, 1, LANES), f32),
            pltpu.VMEM((n_sp, 16, LANES), bf16),
            pltpu.VMEM((n_sp, 16, LANES), bf16),
            pltpu.VMEM((n_sp, 16, LANES), bf16),
            pltpu.VMEM((n_sp, 16, LANES), bf16),
            pltpu.VMEM((n_tp, 2, rows_here, model // 2), bf16),
            pltpu.VMEM((2, rows_here, model // 2), bf16),
            pltpu.VMEM((2, 2, rows_here, model // 2), bf16),
            pltpu.VMEM((rows_here, chunks, LANES), bf16),
            pltpu.VMEM((root_rows * chunks // 2, LANES), f32),
            pltpu.VMEM((n_sp, CAP, chunks, LANES), bf16),
            pltpu.VMEM((2 * n_sp, CAP, chunks, LANES), bf16),
            pltpu.VMEM((root_rows, model), bf16),
            pltpu.VMEM((n_tp, root_rows, hidden), f32),
            pltpu.VMEM((n_tp, root_rows, hidden), bf16),
            pltpu.VMEM((4, 2 * n_sp, CAP, chunks // 4, LANES), bf16),
            pltpu.VMEM((4, n_sp, CAP, chunks // 4, LANES), bf16),
            pltpu.VMEM((n_sp, CAP, chunks // 4, LANES), bf16),
            pltpu.VMEM((3, n_tp, model, hidden), bf16),
            pltpu.VMEM((2, 8, LANES), jnp.int32),
            pltpu.SMEM((8, LANES), jnp.int32),
            pltpu.SMEM((8, LANES), jnp.int32),
            dma((8,)), dma((3,)), dma((3,)), dma((3,)), dma, dma, dma, dma, dma, dma,
            dma((6,)), dma((6,)), dma((9,)), dma((6,)), dma((PLANES + 1,)), dma((4,)), dma, dma((4,)),
        ],
        compiler_params=pltpu.CompilerParams(
            collective_id=0, has_side_effects=True, vmem_limit_bytes=60 * 1024 * 1024
        ),
        name="layer",
    )(
        head_input_values, group_input_vectors, group_readout_vectors, output_gate_values,
        step_size_logits.T, extra_log_decay.T, head_input_filter, input_vector_filter, readout_vector_filter,
        step_size_bias.reshape(1, heads), head_rate_logarithm.reshape(1, heads), direct_path_weight.reshape(1, heads),
        group_norm_scale.astype(f32).reshape(1, width), mixer_output_weight, residual,
        first_norm_scale.reshape(1, model), first_norm_bias.reshape(1, model),
        routes.T, routing_weight.T,
        expert_gate_weight, expert_up_weight, expert_down_weight,
        final_norm_scale.reshape(1, model), final_norm_bias.reshape(1, model),
    )


def solution(mesh):
    in_specs = (
        P("sp", "tp"), P("sp", "tp"), P("sp", "tp"), P("sp", "tp"), P("sp", "tp"), P("sp", "tp"),
        P(None, "tp"), P(None, "tp"), P(None, "tp"), P("tp"), P("tp"), P("tp"), P("tp"),
        P("tp", None), P(("sp", "tp"), None), P(), P(), P(("sp", "tp"), None), P(("sp", "tp"), None),
        P("sp", None, "tp"), P("sp", None, "tp"), P("sp", None, "tp"), P(), P(),
    )
    out_specs = P(("sp", "tp"), None)
    return jax.shard_map(shards, mesh=mesh, in_specs=in_specs, out_specs=out_specs, check_vma=False)
```
